32 devices in a mesh: grp: 2 (over y), sp: 4 (over z), tp: 4 (over x, core).
Axes of the slice: x: 2, y: 2, z: 4, core: 2. Of those that a mesh axis runs over, the one named last changes fastest.
Arguments:
- tokens: bfloat16 [1024, 2048], P(('grp', 'sp')), parts along dimension 0, may hold values from -6 to 6
- norm_gain: float32 [2048], replicated, may hold values from 0.1 to 1.9
- w_query: bfloat16 [2048, 512], P('sp', 'tp'), may hold values from -0.125 to 0.125
- w_key: bfloat16 [2048, 512], P('sp', 'tp'), may hold values from -0.125 to 0.125
- w_value: bfloat16 [2048, 512], P('sp', 'tp'), may hold values from -0.125 to 0.125
- w_glu_value: bfloat16 [2048, 1024], P('sp', 'tp'), may hold values from -0.125 to 0.125
- w_glu_gate: bfloat16 [2048, 1024], P('sp', 'tp'), may hold values from -0.125 to 0.125
- key_offset: bfloat16 [1024, 8], P(('grp', 'sp'), 'tp'), parts along dimension 0, may hold values from -13 to 0
- head_gain: float32 [8, 64], P('tp'), may hold values from 0.1 to 1.9
- conv_taps: float32 [31, 1024], P(None, 'tp'), may hold values from -2.873685 to 2.873685
- channel_gain: float32 [1024], P('tp'), may hold values from 0.1 to 1.9
- channel_bias: float32 [1024], P('tp'), may hold values from -3 to 3
- w_out_attn: bfloat16 [512, 2048], P('tp'), may hold values from -0.15625 to 0.15625
- w_out_conv: bfloat16 [1024, 2048], P('tp'), may hold values from -0.15625 to 0.15625
- out_gain: float32 [2048], replicated, may hold values from 0.1 to 1.9
Outputs:
- mixed: bfloat16 [1024, 2048], P(('grp', 'sp')), parts along dimension 0
- log_mass: float32 [8, 1024], P('tp', ('grp', 'sp')), parts along dimension 1
The draws below stay inside these ranges and needn't reach their ends.
There are 2 independent parts, one for each index of `grp`. The reference program is written for one: setup_inputs(seed, part) draws one part's arguments, and reference() takes and returns one part's arrays. A program takes and returns all parts, laid end to end along the dimension named above; an argument that names none is the same for every part. Nothing has to cross between parts.
All inputs are finite; a program needn't handle non-finite values.
Results may differ from the reference program's by a relative error of at most 0.011.
Values may be sent and summed in bfloat16 or wider, within the bound.
A program may use at most 64 MiB of HBM per device.

```python
import jax
import jax.numpy as jnp
from jax import lax

D = 2048
ATTENTION_HEADS = 8
KVHEADS = 8
HD = 64
CW = 1024
KSIZE = 31
TOKENS = 512


def draw_key_offset(key, part):
    parallel_flows = jax.random.split(jax.random.fold_in(key, 11), 6)
    sequence_length_total = TOKENS
    head_order = jax.random.permutation(parallel_flows[0], ATTENTION_HEADS)
    fast_heads = head_order < ATTENTION_HEADS // 2
    random_noise_values = 0.5 * jax.random.truncated_normal(parallel_flows[1], -4.0, 4.0, (sequence_length_total, ATTENTION_HEADS), jnp.float32)
    slow_base = jnp.log(1.0 / sequence_length_total) - 0.5 - jax.random.uniform(parallel_flows[2], (ATTENTION_HEADS,), jnp.float32, 0.0, 0.5)
    fast_base = jax.random.uniform(parallel_flows[3], (ATTENTION_HEADS,), jnp.float32, -5.0, -4.0)
    head_starting_row = jnp.where(fast_heads, fast_base, slow_base)
    block_count = (sequence_length_total + 127) // 128
    height_levels = jax.random.uniform(parallel_flows[4], (block_count, ATTENTION_HEADS), jnp.float32, -0.7, 0.7)
    height_levels = jnp.repeat(height_levels, 128, axis=0)[:sequence_length_total]
    gathered_key_block = jax.random.split(parallel_flows[5], 2)
    gathered_positions = jax.random.randint(gathered_key_block[0], (4, ATTENTION_HEADS), 0, sequence_length_total)
    token_positions = jnp.arange(sequence_length_total, dtype=jnp.int32)
    broken_stick_mass = jnp.any(token_positions[:, None, None] == gathered_positions[None, :, :], axis=1)
    gathered_value_block = jax.random.uniform(gathered_key_block[1], (sequence_length_total, ATTENTION_HEADS), jnp.float32, -1.4, 0.0)
    final_output = jnp.clip(jnp.where(broken_stick_mass, gathered_value_block, head_starting_row + height_levels + random_noise_values), -13.0, 0.0)
    final_output = final_output.at[0, 0].set(-13.0)
    final_output = final_output.at[0, 1].set(0.0)
    return final_output.astype(jnp.bfloat16)


def draw_conv_taps(key, part):
    stream = jax.random.fold_in(key, 23)
    base_taps = jax.random.truncated_normal(stream, -4.0, 4.0, (KSIZE, CW), jnp.float32)
    channel_rise = jnp.exp(jnp.log(4.0) * jnp.arange(CW, dtype=jnp.float32) / CW)
    return base_taps * channel_rise / jnp.sqrt(float(KSIZE))


def block_scale(key, shape, cuts, smallest, top_value):
    gain, own = 1.0, jax.random.fold_in(key, 6)
    for axis_at, shards_of in cuts:
        steps = jnp.exp(jax.random.uniform(jax.random.fold_in(own, axis_at), (shards_of,), jnp.float32, smallest / len(cuts), top_value / len(cuts)))
        gain = gain * jnp.repeat(steps, shape[axis_at] // shards_of).reshape([-1 if axis == axis_at else 1 for axis in range(len(shape))])
    return gain


def noise(stream_key, dims, scale, reach, pieces=(), kind=jnp.bfloat16):
    values = jax.random.normal(stream_key, dims, jnp.float32) * scale
    if len(pieces) > 0:
        values = block_scale(stream_key, dims, pieces, -0.22, 0.18) * values
    return jnp.clip(values, min=-reach, max=reach).astype(kind)


def setup_inputs(seed: int = 0, part: int = 0) -> dict:
    keys = jax.random.split(jax.random.key(seed), 16)
    own_keys = jax.random.split(jax.random.fold_in(keys[15], part), 16)
    tokens = noise(own_keys[0], (TOKENS, D), 1.0, 6.0, ((0, 4),))
    norm_gain = jnp.clip(1.0 + 0.18 * jax.random.normal(keys[1], (D,), jnp.float32), 0.1, 1.9)
    w_query = noise(keys[2], (D, ATTENTION_HEADS * HD), D ** -0.5, 0.125, ((0, 4), (1, 4)))
    w_key = noise(keys[3], (D, KVHEADS * HD), D ** -0.5, 0.125, ((0, 4), (1, 4)))
    w_value = noise(keys[4], (D, KVHEADS * HD), D ** -0.5, 0.125, ((0, 4), (1, 4)))
    w_glu_value = noise(keys[5], (D, CW), D ** -0.5, 0.125, ((0, 4), (1, 4)))
    w_glu_gate = noise(keys[6], (D, CW), D ** -0.5, 0.125, ((0, 4), (1, 4)))
    key_offset = draw_key_offset(jax.random.fold_in(jax.random.fold_in(keys[15], part), 71), part)
    head_gain = jnp.clip(1.0 + 0.18 * jax.random.normal(keys[8], (ATTENTION_HEADS, HD), jnp.float32), 0.1, 1.9)
    conv_taps = draw_conv_taps(jax.random.fold_in(keys[15], 71), part)
    channel_gain = jnp.clip(1.0 + 0.18 * jax.random.normal(keys[10], (CW,), jnp.float32), 0.1, 1.9)
    channel_bias = noise(keys[11], (CW,), 0.5, 3.0, ((0, 4),), jnp.float32)
    w_out_attn = noise(keys[12], (ATTENTION_HEADS * HD, D), (ATTENTION_HEADS * HD + CW) ** -0.5, 0.15625, ((0, 4),))
    w_out_conv = noise(keys[13], (CW, D), (ATTENTION_HEADS * HD + CW) ** -0.5, 0.15625, ((0, 4),))
    out_gain = jnp.clip(1.0 + 0.18 * jax.random.normal(keys[14], (D,), jnp.float32), 0.1, 1.9)
    return dict(tokens=tokens, norm_gain=norm_gain, w_query=w_query, w_key=w_key, w_value=w_value, w_glu_value=w_glu_value, w_glu_gate=w_glu_gate, key_offset=key_offset, head_gain=head_gain, conv_taps=conv_taps, channel_gain=channel_gain, channel_bias=channel_bias, w_out_attn=w_out_attn, w_out_conv=w_out_conv, out_gain=out_gain)


norm_eps = 1e-06

def row_norm(values_in, gain_vec):
    squares = lax.optimization_barrier(jnp.mean(values_in * values_in, axis=-1, keepdims=True))
    return values_in * lax.rsqrt(squares + norm_eps) * gain_vec

def reference(tokens, norm_gain, w_query, w_key, w_value, w_glu_value, w_glu_gate, key_offset, head_gain, conv_taps, channel_gain, channel_bias, w_out_attn, w_out_conv, out_gain):
    sequence_length_total = tokens.shape[0]
    group_size = ATTENTION_HEADS // KVHEADS
    normed = row_norm(tokens.astype(jnp.float32), norm_gain).astype(jnp.bfloat16)

    def project(weight):
        return jnp.dot(normed, weight, preferred_element_type=jnp.float32).astype(jnp.bfloat16)
    query = project(w_query).astype(jnp.float32).reshape(sequence_length_total, KVHEADS, group_size, HD)
    key_rows = project(w_key).astype(jnp.float32).reshape(sequence_length_total, KVHEADS, HD)
    value_rows = project(w_value).astype(jnp.float32).reshape(sequence_length_total, KVHEADS, HD)
    glu_value = project(w_glu_value)
    glu_gate = project(w_glu_gate)
    offsets = key_offset.astype(jnp.float32).T.reshape(KVHEADS, group_size, 1, sequence_length_total)
    key_pos = jnp.arange(sequence_length_total, dtype=jnp.int32)
    q_block = min(sequence_length_total, 256)

    def attend(first_row):
        q_rows = lax.dynamic_slice_in_dim(query, first_row, q_block, 0)
        scores = jnp.einsum('qhgd,khd->hgqk', q_rows, key_rows) * HD ** (-0.5) + offsets
        query_pos = first_row + jnp.arange(q_block, dtype=jnp.int32)
        allowed = key_pos[None, :] <= query_pos[:, None]
        log_not = jnp.where(allowed, jax.nn.log_sigmoid(-scores), 0.0)
        later = lax.cumsum(log_not, axis=3, reverse=True) - log_not
        weights = jnp.where(allowed, jnp.exp(jax.nn.log_sigmoid(scores) + later), 0.0)
        log_mass = jnp.log(lax.optimization_barrier(jnp.sum(weights, axis=3)))
        rounded = lax.optimization_barrier(weights.astype(jnp.bfloat16)).astype(jnp.float32)
        head_mix = jnp.einsum('hgqk,khd->qhgd', rounded, value_rows)
        return (head_mix, log_mass)
    starts = jnp.arange(0, sequence_length_total, q_block, dtype=jnp.int32)
    head_mix, log_mass = lax.map(attend, starts)
    head_mix = head_mix.reshape(sequence_length_total, ATTENTION_HEADS, HD)
    log_mass = log_mass.transpose(1, 2, 0, 3).reshape(ATTENTION_HEADS, sequence_length_total)
    attended = row_norm(head_mix, head_gain).astype(jnp.bfloat16).reshape(sequence_length_total, ATTENTION_HEADS * HD)
    gated = (glu_value.astype(jnp.float32) * jax.nn.sigmoid(glu_gate.astype(jnp.float32))).astype(jnp.bfloat16)
    padded = jnp.pad(gated.astype(jnp.float32), ((KSIZE - 1, 0), (0, 0)))
    conv_out = jnp.zeros((sequence_length_total, gated.shape[1]), jnp.float32)
    for tap_index in range(KSIZE):
        conv_out = conv_out + conv_taps[tap_index] * padded[tap_index:tap_index + sequence_length_total]
    chan_mean = lax.optimization_barrier(jnp.mean(conv_out, axis=1, keepdims=True))
    centered = conv_out - chan_mean
    spread = lax.optimization_barrier(jnp.mean(centered * centered, axis=1, keepdims=True))
    channel_out = jax.nn.silu(centered * lax.rsqrt(spread + norm_eps) * channel_gain + channel_bias).astype(jnp.bfloat16)
    mix = jnp.dot(attended, w_out_attn, preferred_element_type=jnp.float32) + jnp.dot(channel_out, w_out_conv, preferred_element_type=jnp.float32)
    mixed = row_norm(mix, out_gain).astype(jnp.bfloat16)
    return (mixed, log_mass)
```

```python
import functools

import jax
import jax.numpy as jnp
from jax import lax
from jax.experimental import pallas as pl
from jax.experimental.pallas import tpu as pltpu
from jax.sharding import PartitionSpec as P

HD = 64
CW = 1024


norm_eps = 1e-06


def from_behind(value, axis, steps):
    count = lax.axis_size(axis)
    initial, last = (max(0, -steps), min(count, count - steps))
    return lax.ppermute(value, axis, [(source, source + steps) for source in range(initial, last)])


def row_norm(values_in, gain_vec):
    squares = jnp.mean(values_in * values_in, axis=-1, keepdims=True)
    return values_in * lax.rsqrt(squares + norm_eps) * gain_vec


def local(
    tokens,
    norm_gain,
    w_query,
    w_key,
    w_value,
    w_glu_value,
    w_glu_gate,
    key_offset,
    head_gain,
    conv_taps,
    channel_gain,
    channel_bias,
    w_out_attn,
    w_out_conv,
    out_gain,
):
    row_count = tokens.shape[0]
    normed = row_norm(tokens.astype(jnp.float32), norm_gain).astype(jnp.bfloat16)
    weights_in = (w_query, w_key, w_value, w_glu_value, w_glu_gate)
    pieces = (
        lax.all_gather(weights_in[0], "sp", axis=0, tiled=True),
        lax.all_gather(weights_in[1], "sp", axis=0, tiled=True),
        lax.all_gather(weights_in[2], "sp", axis=0, tiled=True),
        lax.all_gather(weights_in[3], "sp", axis=0, tiled=True),
        lax.all_gather(weights_in[4], "sp", axis=0, tiled=True),
    )
    projected = tuple(
        (jnp.dot(normed, shard_piece, preferred_element_type=jnp.float32) for shard_piece in pieces)
    )
    query, key_rows, value_rows, glu_value, glu_gate = [
        summed.astype(jnp.bfloat16) for summed in projected
    ]
    kv_local = key_rows.shape[1] // HD
    group_size = query.shape[1] // key_rows.shape[1]
    heads_local = kv_local * group_size
    all_keys, all_values, all_offsets = (
        lax.all_gather(key_rows, "sp", axis=0, tiled=True),
        lax.all_gather(value_rows, "sp", axis=0, tiled=True),
        lax.all_gather(key_offset, "sp", axis=0, tiled=True),
    )
    sequence_length_total = all_keys.shape[0]
    shard_count = lax.axis_size("sp")
    per_block = 1
    while (
        per_block * 2 <= shard_count
        and shard_count % (per_block * 2) == 0
        and (per_block * 2 * row_count <= 1024)
    ):
        per_block = per_block * 2
    span_len = per_block * row_count
    query_heads = query.reshape(row_count, kv_local, group_size, HD)
    key_heads = all_keys.reshape(sequence_length_total, kv_local, HD)
    value_heads = all_values.reshape(sequence_length_total, kv_local, HD)
    my_index = lax.axis_index("sp")
    query_pos = my_index * row_count + jnp.arange(row_count, dtype=jnp.int32)
    last_block = my_index // per_block
    zeros_mix = jnp.zeros((kv_local, group_size, row_count, HD), jnp.float32)
    zeros_row = jnp.zeros((kv_local, group_size, row_count), jnp.float32)

    def sweep(turn_index, carry):
        head_mix, mass_sum, carried = carry
        first_key = (last_block - turn_index) * span_len
        key_block = lax.dynamic_slice_in_dim(key_heads, first_key, span_len, 0)
        value_block = lax.dynamic_slice_in_dim(value_heads, first_key, span_len, 0)
        offset_block = lax.dynamic_slice_in_dim(all_offsets, first_key, span_len, 0).astype(
            jnp.float32
        )
        offset_block = offset_block.T.reshape(kv_local, group_size, 1, span_len)
        scores = (
            jnp.einsum("qhgd,khd->hgqk", query_heads, key_block, preferred_element_type=jnp.float32)
            * HD ** (-0.5)
            + offset_block
        )
        key_pos = first_key + jnp.arange(span_len, dtype=jnp.int32)
        allowed = key_pos[None, :] <= query_pos[:, None]
        log_not = jnp.where(allowed, jax.nn.log_sigmoid(-scores), 0.0)
        later = lax.cumsum(log_not, axis=3, reverse=True) - log_not + carried[..., None]
        weights = jnp.where(allowed, jnp.exp(jax.nn.log_sigmoid(scores) + later), 0.0)
        head_mix = head_mix + jnp.einsum(
            "hgqk,khd->hgqd",
            weights.astype(jnp.bfloat16),
            value_block,
            preferred_element_type=jnp.float32,
        )
        return (head_mix, mass_sum + jnp.sum(weights, axis=3), carried + jnp.sum(log_not, axis=3))

    head_mix, mass_sum, leftover = lax.fori_loop(
        0, last_block + 1, sweep, (zeros_mix, zeros_row, zeros_row)
    )
    log_mass = jnp.log(mass_sum).reshape(heads_local, row_count)
    head_rows = head_mix.transpose(2, 0, 1, 3).reshape(row_count, heads_local, HD)
    attended = (
        row_norm(head_rows, head_gain).astype(jnp.bfloat16).reshape(row_count, heads_local * HD)
    )
    gated = (glu_value.astype(jnp.float32) * jax.nn.sigmoid(glu_gate.astype(jnp.float32))).astype(
        jnp.bfloat16
    )
    reach_len = conv_taps.shape[0] - 1
    before = from_behind(gated[row_count - reach_len :], "sp", 1)
    padded = jnp.concatenate([before, gated], axis=0).astype(jnp.float32)
    conv_out = jnp.zeros(gated.shape, jnp.float32)
    for tap_index in range(conv_taps.shape[0]):
        conv_out = conv_out + conv_taps[tap_index] * padded[tap_index : tap_index + row_count]
    total_sum, total_squares = lax.psum(
        (jnp.sum(conv_out, axis=1), jnp.sum(conv_out * conv_out, axis=1)), "tp"
    )
    chan_mean = (total_sum / CW)[:, None]
    spread = (total_squares / CW)[:, None] - chan_mean * chan_mean
    centered = conv_out - chan_mean
    channel_out = jax.nn.silu(
        centered * lax.rsqrt(spread + norm_eps) * channel_gain + channel_bias
    ).astype(jnp.bfloat16)
    share = lax.psum_scatter(
        jnp.dot(attended, w_out_attn, preferred_element_type=jnp.float32)
        + jnp.dot(channel_out, w_out_conv, preferred_element_type=jnp.float32),
        "tp",
        scatter_dimension=0,
        tiled=True,
    )
    mixed = lax.all_gather(row_norm(share, out_gain).astype(jnp.bfloat16), "tp", axis=0, tiled=True)
    return (mixed, log_mass)


F32 = jnp.float32
BF16 = jnp.bfloat16
MESH = pl.DeviceIdType.MESH


def split_kernel(
    SP,
    tokens,
    norm_gain,
    w_query,
    w_key,
    w_value,
    w_gv,
    w_gg,
    key_offset,
    head_gain,
    conv_taps,
    channel_gain,
    channel_bias,
    w_oa,
    w_oc,
    out_gain,
    out,
    log_out,
    X,
    WA,
    stg,
    prm,
    offs,
    offr,
    proj,
    gp,
    snd,
    lms,
    sts,
    ar,
    cr,
    lmr,
    sr,
    woa,
    woc,
    mp,
    ma,
    bx,
    bxr,
    s_wo,
    s_ws,
    s_wr,
    s_wys,
    s_wyr,
    s_xl,
    s_xrt,
    s_xr,
    s_xxs,
    s_xxr,
    s_xds,
    s_xdr,
    s_ps,
    s_pr,
    s_os,
    s_or,
    s_ds,
    s_dr,
    s_ls,
    s_lr,
    s_ss,
    s_sr,
    s_ms,
    s_mr,
    s_bs,
    s_br,
    s_es,
    s_er,
):
    g = lax.axis_index("grp")
    z = lax.axis_index("sp")
    tp = lax.axis_index("tp")
    x = tp // 2
    c = tp % 2
    partner = 2 * x + (1 - c)
    across = 2 * (1 - x) + c
    diag = 2 * (1 - x) + (1 - c)
    mine = z // 2
    par = z % 2
    R = tokens.shape[0]
    D = tokens.shape[1]
    KS = w_query.shape[0]
    KH = KS // 2
    Q = R // 4
    taps_n = conv_taps.shape[0]

    def rc(src, dst, ss, rs, dev):
        return pltpu.make_async_remote_copy(
            src_ref=src, dst_ref=dst, send_sem=ss, recv_sem=rs, device_id=dev, device_id_type=MESH
        )

    wo_a = pltpu.make_async_copy(w_oa, woa, s_wo.at[0])
    wo_c = pltpu.make_async_copy(w_oc, woc, s_wo.at[1])
    wo_a.start()
    wo_c.start()

    barrier = pltpu.get_barrier_semaphore()
    for dz in range(SP):
        for dt in range(4):
            if dz == 0 and dt == 0:
                continue
            pl.semaphore_signal(
                barrier, inc=1, device_id=(g, (z + dz) % SP, (tp + dt) % 4), device_id_type=MESH
            )
    pl.semaphore_signal(barrier, inc=1, device_id=(1 - g, z, tp), device_id_type=MESH)

    t32 = tokens[...].astype(F32)
    sq = jnp.mean(t32 * t32, axis=-1, keepdims=True)
    X[pl.ds(pl.multiple_of(z * R, R), R), :] = (
        t32 * lax.rsqrt(sq + norm_eps) * norm_gain[...]
    ).astype(BF16)
    pl.semaphore_wait(barrier, SP * 4)

    def xs(block, quarter):
        return X.at[pl.ds(pl.multiple_of(block * R + quarter * Q, Q), Q), :]

    def x_right(b):
        return rc(xs(b, tp), xs(b, tp), s_xrt.at[b], s_xr.at[b], (g, jnp.minimum(z + 1, SP - 1), tp))

    def x_left(b):
        return rc(xs(b, tp), xs(b, tp), s_xl.at[b], s_xr.at[b], (g, jnp.maximum(z - 1, 0), tp))

    def x_cross(b):
        return rc(xs(b, tp), xs(b, tp), s_xxs.at[b], s_xxr.at[b], (g, z, across))

    def x_cross_in(b):
        return rc(xs(b, across), xs(b, across), s_xxs.at[b], s_xxr.at[b], (g, z, across))

    def x_d2d(b, k, quarter):
        return rc(xs(b, quarter), xs(b, quarter), s_xds.at[b, k], s_xdr.at[b, k], (g, z, partner))

    @pl.when(z < SP - 1)
    def _():
        x_right(z).start()

    @pl.when(z > 0)
    def _():
        x_left(z).start()

    for h in range(2):
        stg[h, 0, :, 0:128] = jnp.concatenate(
            [w_query[:, 64 * h : 64 * h + 64], w_key[:, 64 * h : 64 * h + 64]], axis=1
        )
        stg[h, 0, :, 128:256] = w_value[...]
        stg[h, 1, :, 0:128] = w_gv[:, 128 * h : 128 * h + 128]
        stg[h, 1, :, 128:256] = w_gg[:, 128 * h : 128 * h + 128]

    def w_half(b, part):
        return WA.at[pl.ds(pl.multiple_of(b * KS + part * KH, KH), KH), :]

    def w_full(b):
        return WA.at[pl.ds(pl.multiple_of(b * KS, KS), KS), :]

    def w_far(h, r):
        return rc(
            stg.at[h, r, pl.ds(pl.multiple_of(g * KH, KH), KH), :],
            w_half(z, g),
            s_ws.at[h, r],
            s_wr.at[z],
            (g, 2 * c + h, 2 * x + r),
        )

    def w_near(h, r):
        return rc(stg.at[h, r], w_full(z), s_ws.at[h, r], s_wr.at[z], (g, z, partner))

    def w_own(h, r):
        return pltpu.make_async_copy(stg.at[h, r], w_full(z), s_wr.at[z])

    for h in range(2):
        for r in range(2):
            zt = 2 * c + h

            @pl.when(zt != z)
            def _():
                w_far(h, r).start()

            @pl.when((zt == z) & (c != r))
            def _():
                w_near(h, r).start()

            @pl.when((zt == z) & (c == r))
            def _():
                w_own(h, r).start()

    eye = lax.broadcasted_iota(jnp.int32, (R, R), 0) == lax.broadcasted_iota(jnp.int32, (R, R), 1)

    def to_row(col):
        return jnp.broadcast_to(
            jnp.sum(jnp.where(eye, jnp.broadcast_to(col, (R, R)), 0.0), axis=0, keepdims=True), (8, R)
        )

    def to_col(row):
        return jnp.sum(jnp.where(eye, jnp.broadcast_to(row, (R, R)), 0.0), axis=1, keepdims=True)

    def off_far(h):
        return rc(offs.at[h], offr.at[z], s_os.at[h], s_or.at[z], (g, 2 * c + h, 2 * x))

    def off_own(h):
        return pltpu.make_async_copy(offs.at[h], offr.at[z], s_or.at[z])

    ko = key_offset[...].astype(F32)
    for h in range(2):
        offs[h] = to_row(ko[:, h : h + 1])
        own = (2 * c + h == z) & (c == 0)

        @pl.when(own)
        def _():
            off_own(h).start()

        @pl.when(jnp.logical_not(own))
        def _():
            off_far(h).start()

    p_send = rc(prm, prm, s_ps.at[0], s_pr.at[0], (g, z, partner))

    @pl.when(c == mine)
    def _():
        tt = jnp.where(par == 0, conv_taps[:, 0:128], conv_taps[:, 128:256])
        prm[0:taps_n, :] = tt
        prm[32:33, :] = jnp.concatenate([head_gain[0:1, :], head_gain[1:2, :]], axis=1)
        p_send.start()

    for d in range(1, SP):

        @pl.when(z - d >= 0)
        def _():
            b = z - d
            x_left(b).wait_recv()

            @pl.when(z < SP - 1)
            def _():
                x_right(b).start()

            x_cross(b).start()
            x_d2d(b, 0, tp).start()

        @pl.when(z + d < SP)
        def _():
            b = z + d
            x_left(b).wait_recv()

            @pl.when(z > 0)
            def _():
                x_left(b).start()

            x_cross(b).start()
            x_d2d(b, 0, tp).start()

        for sgn in (-1, 1):

            @pl.when((z + sgn * d >= 0) & (z + sgn * d < SP))
            def _():
                b = z + sgn * d
                x_cross_in(b).wait_recv()
                x_d2d(b, 1, across).start()

        for sgn in (-1, 1):

            @pl.when((z + sgn * d >= 0) & (z + sgn * d < SP))
            def _():
                b = z + sgn * d
                w = rc(w_half(b, g), w_half(b, g), s_wys.at[b], s_wr.at[b], (1 - g, z, tp))
                w.wait_recv()
                rc(w_half(b, g), w_half(b, g), s_wys.at[b], s_wyr.at[b], (1 - g, z, tp)).start()

    @pl.when(c == mine)
    def _():
        pltpu.make_async_copy(w_full(z), w_full(z), s_wr.at[z]).wait()

    @pl.when(c != mine)
    def _():
        rc(w_full(z), w_full(z), s_ws.at[0, 0], s_wr.at[z], (g, z, partner)).wait_recv()
        p_send.wait_recv()

    for d in range(1, SP):
        for sgn in (-1, 1):

            @pl.when((z + sgn * d >= 0) & (z + sgn * d < SP))
            def _():
                b = z + sgn * d
                x_d2d(b, 0, partner).wait_recv()
                x_d2d(b, 1, diag).wait_recv()
                rc(
                    w_half(b, 1 - g), w_half(b, 1 - g), s_wys.at[b], s_wyr.at[b], (1 - g, z, tp)
                ).wait_recv()

    for b in range(SP):
        proj[b * R : b * R + R, :] = jnp.dot(
            X[b * R : b * R + R, :], WA[...], preferred_element_type=F32
        ).astype(BF16)

    def d_far(t, core):
        buf = ar if core == 0 else cr
        return rc(snd.at[t], buf.at[par], s_ds.at[t], s_dr.at[core, par], (g, t, 2 * x + mine))

    def d_own(t, core):
        buf = ar if core == 0 else cr
        return pltpu.make_async_copy(snd.at[t], buf.at[par], s_dr.at[core, par])

    def l_far(t):
        return rc(lms.at[t], lmr.at[par], s_ls.at[t], s_lr.at[par], (g, t, 2 * x + mine))

    def l_own(t):
        return pltpu.make_async_copy(lms.at[t], lmr.at[par], s_lr.at[par])

    def s_far(t, q):
        return rc(sts.at[t], sr.at[4 * x + z], s_ss.at[t, q], s_sr.at[4 * x + z], (g, t, q))

    def s_own(t):
        return pltpu.make_async_copy(sts.at[t], sr.at[4 * x + z], s_sr.at[4 * x + z])

    @pl.when(c == 0)
    def _():
        for s in range(SP):
            own = (s == z) & (mine == 0)

            @pl.when(own)
            def _():
                pltpu.make_async_copy(offr.at[s], offr.at[s], s_or.at[s]).wait()

            @pl.when(jnp.logical_not(own))
            def _():
                rc(offr.at[s], offr.at[s], s_os.at[0], s_or.at[s], (g, z, partner)).wait_recv()

        row_i = lax.broadcasted_iota(jnp.int32, (R, R), 0)
        col_i = lax.broadcasted_iota(jnp.int32, (R, R), 1)
        upper = jnp.where(row_i >= col_i, 1.0, 0.0).astype(BF16)
        allowed = col_i <= row_i
        lane_ok = (lax.broadcasted_iota(jnp.int32, (R, 128), 1) // 64) == par
        for b in range(SP - 1, -1, -1):
            q = proj[b * R : b * R + R, 0:64]
            acc = jnp.zeros((R, 128), F32)
            mass = jnp.zeros((R, 1), F32)
            carried = jnp.zeros((R, 1), F32)
            for kb in range(b, -1, -1):
                k = proj[kb * R : kb * R + R, 64:128]
                v = proj[kb * R : kb * R + R, 128:256]
                v = jnp.where(lane_ok, v.astype(F32), 0.0).astype(BF16)
                s = (
                    lax.dot_general(q, k, (((1,), (1,)), ((), ())), preferred_element_type=F32)
                    * HD ** (-0.5)
                    + offr[kb, 0:1, :]
                )
                ln = -(jnp.maximum(s, 0.0) + jnp.log1p(jnp.exp(-jnp.abs(s))))
                if kb == b:
                    ln = jnp.where(allowed, ln, 0.0)
                hi = ln.astype(BF16)
                lo = (ln - hi.astype(F32)).astype(BF16)
                incl = (
                    jnp.dot(hi, upper, preferred_element_type=F32)
                    + jnp.dot(lo, upper, preferred_element_type=F32)
                    + carried
                )
                w = jnp.exp(s + incl)
                if kb == b:
                    w = jnp.where(allowed, w, 0.0)
                carried = incl[:, 0:1]
                mass = mass + jnp.sum(w, axis=1, keepdims=True)
                acc = acc + jnp.dot(w.astype(BF16), v, preferred_element_type=F32)
            ms = jnp.sum(acc * acc, axis=1, keepdims=True) / 64
            snd[b] = (acc * lax.rsqrt(ms + norm_eps) * prm[32:33, :]).astype(BF16)
            lms[b] = jnp.log(to_row(mass))
            own = (b == z) & (mine == 0)

            @pl.when(own)
            def _():
                d_own(b, 0).start()
                l_own(b).start()

            @pl.when(jnp.logical_not(own))
            def _():
                d_far(b, 0).start()
                l_far(b).start()

    @pl.when(c == 1)
    def _():
        gp[0:32, :] = jnp.zeros((32, 128), F32)
        gv = proj[:, 0:128].astype(F32)
        gg = proj[:, 128:256].astype(F32)
        gp[32 : 32 + SP * R, :] = (gv * jax.nn.sigmoid(gg)).astype(BF16).astype(F32)
        for b in range(SP):
            conv = jnp.zeros((R, 128), F32)
            for j in range(taps_n):
                first = b * R + 32 - (taps_n - 1) + j
                conv = conv + prm[j : j + 1, :] * gp[first : first + R, :]
            snd[b] = conv.astype(BF16)
            sts[b, 0] = to_row(jnp.sum(conv, axis=1, keepdims=True))
            sts[b, 1] = to_row(jnp.sum(conv * conv, axis=1, keepdims=True))
            own = (b == z) & (mine == 1)

            @pl.when(own)
            def _():
                d_own(b, 1).start()

            @pl.when(jnp.logical_not(own))
            def _():
                d_far(b, 1).start()

            for q in range(4):
                self_st = (b == z) & (q == tp)

                @pl.when(self_st)
                def _():
                    s_own(b).start()

                @pl.when(jnp.logical_not(self_st))
                def _():
                    s_far(b, q).start()

    for h in range(2):
        zs = 2 * c + h
        for core in range(2):
            buf = ar if core == 0 else cr
            own = (zs == z) & (c == core)

            @pl.when(own)
            def _():
                pltpu.make_async_copy(buf.at[h], buf.at[h], s_dr.at[core, h]).wait()
                if core == 0:
                    pltpu.make_async_copy(lmr.at[h], lmr.at[h], s_lr.at[h]).wait()

            @pl.when(jnp.logical_not(own))
            def _():
                rc(buf.at[h], buf.at[h], s_ds.at[0], s_dr.at[core, h], (g, z, partner)).wait_recv()
                if core == 0:
                    rc(lmr.at[h], lmr.at[h], s_ls.at[0], s_lr.at[h], (g, z, partner)).wait_recv()

    for xx in range(2):
        for s in range(SP):
            i = 4 * xx + s
            own = (s == z) & (xx == x) & (c == 1)

            @pl.when(own)
            def _():
                pltpu.make_async_copy(sr.at[i], sr.at[i], s_sr.at[i]).wait()

            @pl.when(jnp.logical_not(own))
            def _():
                rc(sr.at[i], sr.at[i], s_ss.at[0, 0], s_sr.at[i], (g, z, partner)).wait_recv()

    log_out[0:1, :] = lmr[0, 0:1, :]
    log_out[1:2, :] = lmr[1, 0:1, :]
    tot = sr[0]
    for i in range(1, 2 * SP):
        tot = tot + sr[i]
    mean = to_col(tot[0, 0:1, :]) / CW
    spread = to_col(tot[1, 0:1, :]) / CW - mean * mean
    inv = lax.rsqrt(spread + norm_eps)
    att = ar[0] + ar[1]
    chans = []
    for h in range(2):
        v = (cr[h].astype(F32) - mean) * inv * channel_gain[:, 128 * h : 128 * h + 128] + channel_bias[
            :, 128 * h : 128 * h + 128
        ]
        chans.append((v * jax.nn.sigmoid(v)).astype(BF16))
    feats = jnp.concatenate([att] + chans, axis=1)
    wo_a.wait()
    wo_c.wait()
    H = R // 2
    n_col = 4
    cw = D // n_col
    for k in range(n_col):
        cs = slice(k * cw, (k + 1) * cw)
        mp[:, cs] = jnp.dot(feats[:, 0:128], woa[:, cs], preferred_element_type=F32) + jnp.dot(
            feats[:, 128:384], woc[:, cs], preferred_element_type=F32
        )
    away = pl.ds(pl.multiple_of((1 - c) * H, H), H)
    here = pl.ds(pl.multiple_of(c * H, H), H)
    m_send = rc(mp.at[away, :], ma, s_ms.at[0], s_mr.at[0], (g, z, partner))
    m_send.start()
    m_send.wait_recv()
    bx[...] = (mp[here, :] + ma[...]).astype(BF16)
    b_send = rc(bx, bxr, s_bs.at[0], s_br.at[0], (g, z, across))
    b_send.start()
    b_send.wait_recv()
    tot2 = bx[...].astype(F32) + bxr[...].astype(F32)
    ms = jnp.mean(tot2 * tot2, axis=-1, keepdims=True)
    out[here, :] = (tot2 * lax.rsqrt(ms + norm_eps) * out_gain[...]).astype(BF16)
    e_send = rc(out.at[here, :], out.at[here, :], s_es.at[0], s_er.at[0], (g, z, partner))
    e_send.start()

    @pl.when(z < SP - 1)
    def _():
        x_right(z).wait_send()

    @pl.when(z > 0)
    def _():
        x_left(z).wait_send()

    for d in range(1, SP):

        @pl.when(z - d >= 0)
        def _():
            b = z - d

            @pl.when(z < SP - 1)
            def _():
                x_right(b).wait_send()

        @pl.when(z + d < SP)
        def _():
            b = z + d

            @pl.when(z > 0)
            def _():
                x_left(b).wait_send()

        for sgn in (-1, 1):

            @pl.when((z + sgn * d >= 0) & (z + sgn * d < SP))
            def _():
                b = z + sgn * d
                x_cross(b).wait_send()
                x_d2d(b, 0, tp).wait_send()
                x_d2d(b, 1, across).wait_send()
                rc(
                    w_half(b, g), w_half(b, g), s_wys.at[b], s_wyr.at[b], (1 - g, z, tp)
                ).wait_send()

    for h in range(2):
        for r in range(2):
            zt = 2 * c + h

            @pl.when(zt != z)
            def _():
                w_far(h, r).wait_send()

            @pl.when((zt == z) & (c != r))
            def _():
                w_near(h, r).wait_send()

        own = (2 * c + h == z) & (c == 0)

        @pl.when(jnp.logical_not(own))
        def _():
            off_far(h).wait_send()

    @pl.when(c == mine)
    def _():
        p_send.wait_send()

    for t in range(SP):
        for core in range(2):

            @pl.when((c == core) & jnp.logical_not((t == z) & (mine == core)))
            def _():
                d_far(t, core).wait_send()
                if core == 0:
                    l_far(t).wait_send()

        for q in range(4):

            @pl.when((c == 1) & jnp.logical_not((t == z) & (q == tp)))
            def _():
                s_far(t, q).wait_send()

    m_send.wait_send()
    b_send.wait_send()
    e_send.wait()


def split_local(
    tokens,
    norm_gain,
    w_query,
    w_key,
    w_value,
    w_gv,
    w_gg,
    key_offset,
    head_gain,
    conv_taps,
    channel_gain,
    channel_bias,
    w_oa,
    w_oc,
    out_gain,
):
    SP = lax.axis_size("sp")
    R, D = tokens.shape
    KS = w_query.shape[0]
    DMA = pltpu.SemaphoreType.DMA
    vm = pl.BlockSpec(memory_space=pltpu.VMEM)
    hb = pl.BlockSpec(memory_space=pl.ANY)
    V = pltpu.VMEM
    return pl.pallas_call(
        functools.partial(split_kernel, SP),
        out_shape=(
            jax.ShapeDtypeStruct((R, D), BF16),
            jax.ShapeDtypeStruct((2, R), F32),
        ),
        in_specs=[vm] * 12 + [hb, hb, vm],
        out_specs=(vm, vm),
        scratch_shapes=[
            V((SP * R, D), BF16),
            V((SP * KS, 256), BF16),
            V((2, 2, KS, 256), BF16),
            V((40, 128), F32),
            V((2, 8, R), F32),
            V((SP, 8, R), F32),
            V((SP * R, 256), BF16),
            V((SP * R + 32, 128), F32),
            V((SP, R, 128), BF16),
            V((SP, 8, R), F32),
            V((SP, 2, 8, R), F32),
            V((2, R, 128), BF16),
            V((2, R, 128), BF16),
            V((2, 8, R), F32),
            V((2 * SP, 2, 8, R), F32),
            V(w_oa.shape, BF16),
            V(w_oc.shape, BF16),
            V((R, D), F32),
            V((R // 2, D), F32),
            V((R // 2, D), BF16),
            V((R // 2, D), BF16),
            DMA((2,)),
            DMA((2, 2)),
            DMA((SP,)),
            DMA((SP,)),
            DMA((SP,)),
            DMA((SP,)),
            DMA((SP,)),
            DMA((SP,)),
            DMA((SP,)),
            DMA((SP,)),
            DMA((SP, 2)),
            DMA((SP, 2)),
            DMA((1,)),
            DMA((1,)),
            DMA((2,)),
            DMA((SP,)),
            DMA((SP,)),
            DMA((2, 2)),
            DMA((SP,)),
            DMA((2,)),
            DMA((SP, 4)),
            DMA((2 * SP,)),
            DMA((1,)),
            DMA((1,)),
            DMA((1,)),
            DMA((1,)),
            DMA((1,)),
            DMA((1,)),
        ],
        compiler_params=pltpu.CompilerParams(collective_id=0, has_side_effects=True),
    )(
        tokens,
        norm_gain.reshape(1, -1),
        w_query,
        w_key,
        w_value,
        w_gv,
        w_gg,
        key_offset,
        head_gain,
        conv_taps,
        channel_gain.reshape(1, -1),
        channel_bias.reshape(1, -1),
        w_oa,
        w_oc,
        out_gain.reshape(1, -1),
    )


def either(*args):
    tokens, w_query, head_gain, conv_taps = args[0], args[2], args[8], args[9]
    fits = (
        lax.axis_size("grp") == 2
        and lax.axis_size("sp") == 4
        and lax.axis_size("tp") == 4
        and tokens.shape[0] == 128
        and w_query.shape[0] * 4 == tokens.shape[1]
        and head_gain.shape == (2, 64)
        and conv_taps.shape[1] == 256
        and conv_taps.shape[0] <= 32
        and args[3].shape[1] == 128
    )
    return split_local(*args) if fits else local(*args)


def solution(mesh):
    in_specs = (
        P(("grp", "sp"), None),
        P(),
        P("sp", "tp"),
        P("sp", "tp"),
        P("sp", "tp"),
        P("sp", "tp"),
        P("sp", "tp"),
        P(("grp", "sp"), "tp"),
        P("tp", None),
        P(None, "tp"),
        P("tp"),
        P("tp"),
        P("tp", None),
        P("tp", None),
        P(),
    )
    out_specs = (P(("grp", "sp"), None), P("tp", ("grp", "sp")))
    return jax.shard_map(either, mesh=mesh, in_specs=in_specs, out_specs=out_specs, check_vma=False)
```

```python
import functools

import jax
import jax.numpy as jnp
from jax import lax
from jax.experimental import pallas as pl
from jax.experimental.pallas import tpu as pltpu
from jax.sharding import PartitionSpec as P

HD = 64
CW = 1024


norm_eps = 1e-06


def from_behind(value, axis, steps):
    count = lax.axis_size(axis)
    initial, last = (max(0, -steps), min(count, count - steps))
    return lax.ppermute(value, axis, [(source, source + steps) for source in range(initial, last)])


def row_norm(values_in, gain_vec):
    squares = jnp.mean(values_in * values_in, axis=-1, keepdims=True)
    return values_in * lax.rsqrt(squares + norm_eps) * gain_vec


def local(
    tokens,
    norm_gain,
    w_query,
    w_key,
    w_value,
    w_glu_value,
    w_glu_gate,
    key_offset,
    head_gain,
    conv_taps,
    channel_gain,
    channel_bias,
    w_out_attn,
    w_out_conv,
    out_gain,
):
    row_count = tokens.shape[0]
    normed = row_norm(tokens.astype(jnp.float32), norm_gain).astype(jnp.bfloat16)
    weights_in = (w_query, w_key, w_value, w_glu_value, w_glu_gate)
    pieces = (
        lax.all_gather(weights_in[0], "sp", axis=0, tiled=True),
        lax.all_gather(weights_in[1], "sp", axis=0, tiled=True),
        lax.all_gather(weights_in[2], "sp", axis=0, tiled=True),
        lax.all_gather(weights_in[3], "sp", axis=0, tiled=True),
        lax.all_gather(weights_in[4], "sp", axis=0, tiled=True),
    )
    projected = tuple(
        (jnp.dot(normed, shard_piece, preferred_element_type=jnp.float32) for shard_piece in pieces)
    )
    query, key_rows, value_rows, glu_value, glu_gate = [
        summed.astype(jnp.bfloat16) for summed in projected
    ]
    kv_local = key_rows.shape[1] // HD
    group_size = query.shape[1] // key_rows.shape[1]
    heads_local = kv_local * group_size
    all_keys, all_values, all_offsets = (
        lax.all_gather(key_rows, "sp", axis=0, tiled=True),
        lax.all_gather(value_rows, "sp", axis=0, tiled=True),
        lax.all_gather(key_offset, "sp", axis=0, tiled=True),
    )
    sequence_length_total = all_keys.shape[0]
    shard_count = lax.axis_size("sp")
    per_block = 1
    while (
        per_block * 2 <= shard_count
        and shard_count % (per_block * 2) == 0
        and (per_block * 2 * row_count <= 1024)
    ):
        per_block = per_block * 2
    span_len = per_block * row_count
    query_heads = query.reshape(row_count, kv_local, group_size, HD)
    key_heads = all_keys.reshape(sequence_length_total, kv_local, HD)
    value_heads = all_values.reshape(sequence_length_total, kv_local, HD)
    my_index = lax.axis_index("sp")
    query_pos = my_index * row_count + jnp.arange(row_count, dtype=jnp.int32)
    last_block = my_index // per_block
    zeros_mix = jnp.zeros((kv_local, group_size, row_count, HD), jnp.float32)
    zeros_row = jnp.zeros((kv_local, group_size, row_count), jnp.float32)

    def sweep(turn_index, carry):
        head_mix, mass_sum, carried = carry
        first_key = (last_block - turn_index) * span_len
        key_block = lax.dynamic_slice_in_dim(key_heads, first_key, span_len, 0)
        value_block = lax.dynamic_slice_in_dim(value_heads, first_key, span_len, 0)
        offset_block = lax.dynamic_slice_in_dim(all_offsets, first_key, span_len, 0).astype(
            jnp.float32
        )
        offset_block = offset_block.T.reshape(kv_local, group_size, 1, span_len)
        scores = (
            jnp.einsum("qhgd,khd->hgqk", query_heads, key_block, preferred_element_type=jnp.float32)
            * HD ** (-0.5)
            + offset_block
        )
        key_pos = first_key + jnp.arange(span_len, dtype=jnp.int32)
        allowed = key_pos[None, :] <= query_pos[:, None]
        log_not = jnp.where(allowed, jax.nn.log_sigmoid(-scores), 0.0)
        later = lax.cumsum(log_not, axis=3, reverse=True) - log_not + carried[..., None]
        weights = jnp.where(allowed, jnp.exp(jax.nn.log_sigmoid(scores) + later), 0.0)
        head_mix = head_mix + jnp.einsum(
            "hgqk,khd->hgqd",
            weights.astype(jnp.bfloat16),
            value_block,
            preferred_element_type=jnp.float32,
        )
        return (head_mix, mass_sum + jnp.sum(weights, axis=3), carried + jnp.sum(log_not, axis=3))

    head_mix, mass_sum, leftover = lax.fori_loop(
        0, last_block + 1, sweep, (zeros_mix, zeros_row, zeros_row)
    )
    log_mass = jnp.log(mass_sum).reshape(heads_local, row_count)
    head_rows = head_mix.transpose(2, 0, 1, 3).reshape(row_count, heads_local, HD)
    attended = (
        row_norm(head_rows, head_gain).astype(jnp.bfloat16).reshape(row_count, heads_local * HD)
    )
    gated = (glu_value.astype(jnp.float32) * jax.nn.sigmoid(glu_gate.astype(jnp.float32))).astype(
        jnp.bfloat16
    )
    reach_len = conv_taps.shape[0] - 1
    before = from_behind(gated[row_count - reach_len :], "sp", 1)
    padded = jnp.concatenate([before, gated], axis=0).astype(jnp.float32)
    conv_out = jnp.zeros(gated.shape, jnp.float32)
    for tap_index in range(conv_taps.shape[0]):
        conv_out = conv_out + conv_taps[tap_index] * padded[tap_index : tap_index + row_count]
    total_sum, total_squares = lax.psum(
        (jnp.sum(conv_out, axis=1), jnp.sum(conv_out * conv_out, axis=1)), "tp"
    )
    chan_mean = (total_sum / CW)[:, None]
    spread = (total_squares / CW)[:, None] - chan_mean * chan_mean
    centered = conv_out - chan_mean
    channel_out = jax.nn.silu(
        centered * lax.rsqrt(spread + norm_eps) * channel_gain + channel_bias
    ).astype(jnp.bfloat16)
    share = lax.psum_scatter(
        jnp.dot(attended, w_out_attn, preferred_element_type=jnp.float32)
        + jnp.dot(channel_out, w_out_conv, preferred_element_type=jnp.float32),
        "tp",
        scatter_dimension=0,
        tiled=True,
    )
    mixed = lax.all_gather(row_norm(share, out_gain).astype(jnp.bfloat16), "tp", axis=0, tiled=True)
    return (mixed, log_mass)


F32 = jnp.float32
BF16 = jnp.bfloat16
MESH = pl.DeviceIdType.MESH


def split_kernel(
    SP,
    tokens,
    norm_gain,
    w_query,
    w_key,
    w_value,
    w_gv,
    w_gg,
    key_offset,
    head_gain,
    conv_taps,
    channel_gain,
    channel_bias,
    w_oa,
    w_oc,
    out_gain,
    out,
    log_out,
    X,
    WA,
    stg,
    prm,
    offs,
    offr,
    proj,
    gp,
    snd,
    lms,
    sts,
    ar,
    cr,
    lmr,
    sr,
    woa,
    woc,
    mp,
    ma,
    bx,
    bxr,
    s_wo,
    s_ws,
    s_wr,
    s_wys,
    s_wyr,
    s_xl,
    s_xrt,
    s_xr,
    s_xxs,
    s_xxr,
    s_xds,
    s_xdr,
    s_ps,
    s_pr,
    s_os,
    s_or,
    s_ds,
    s_dr,
    s_ls,
    s_lr,
    s_ss,
    s_sr,
    s_ms,
    s_mr,
    s_bs,
    s_br,
    s_es,
    s_er,
    tokv,
    wqv,
    wkv,
    s_in,
):
    g = lax.axis_index("grp")
    z = lax.axis_index("sp")
    tp = lax.axis_index("tp")
    x = tp // 2
    c = tp % 2
    partner = 2 * x + (1 - c)
    across = 2 * (1 - x) + c
    diag = 2 * (1 - x) + (1 - c)
    mine = z // 2
    par = z % 2
    NS = 2
    R = tokens.shape[0]
    D = tokens.shape[1]
    KS = w_query.shape[0]
    KH = KS // 2
    Q = R // 4
    taps_n = conv_taps.shape[0]

    def rc(src, dst, ss, rs, dev):
        return pltpu.make_async_remote_copy(
            src_ref=src, dst_ref=dst, send_sem=ss, recv_sem=rs, device_id=dev, device_id_type=MESH
        )

    def cp(src, dst, i):
        return pltpu.make_async_copy(src, dst, s_in.at[i])

    in_tok = cp(tokens, tokv, 0)
    in_q = cp(w_query, wqv, 1)
    in_k = cp(w_key, wkv, 2)
    in_w = []
    for h in range(2):
        lanes = slice(128 * h, 128 * h + 128)
        in_w.append(cp(w_value, stg.at[h, 0, :, 128:256], 3 + 3 * h))
        in_w.append(cp(w_gv.at[:, lanes], stg.at[h, 1, :, 0:128], 4 + 3 * h))
        in_w.append(cp(w_gg.at[:, lanes], stg.at[h, 1, :, 128:256], 5 + 3 * h))
    wo_a = pltpu.make_async_copy(w_oa, woa, s_wo.at[0])
    wo_c = pltpu.make_async_copy(w_oc, woc, s_wo.at[1])
    for copy in [in_tok, in_q, in_k] + in_w + [wo_a, wo_c]:
        copy.start()

    barrier = pltpu.get_barrier_semaphore()
    for dz in range(SP):
        for dt in range(4):
            if dz == 0 and dt == 0:
                continue
            pl.semaphore_signal(
                barrier, inc=1, device_id=(g, (z + dz) % SP, (tp + dt) % 4), device_id_type=MESH
            )
    pl.semaphore_signal(barrier, inc=1, device_id=(1 - g, z, tp), device_id_type=MESH)

    in_tok.wait()
    t32 = tokv[...].astype(F32)
    sq = jnp.mean(t32 * t32, axis=-1, keepdims=True)
    X[pl.ds(pl.multiple_of(z * R, R), R), :] = (
        t32 * lax.rsqrt(sq + norm_eps) * norm_gain[...]
    ).astype(BF16)
    pl.semaphore_wait(barrier, SP * 4)

    QS = Q // NS

    def xs(block, quarter, u):
        return X.at[pl.ds(pl.multiple_of(block * R + quarter * Q + u * QS, QS), QS), :]

    def x_right(b, u):
        r = xs(b, tp, u)
        return rc(r, r, s_xrt.at[b, u], s_xr.at[b, u], (g, jnp.minimum(z + 1, SP - 1), tp))

    def x_left(b, u):
        r = xs(b, tp, u)
        return rc(r, r, s_xl.at[b, u], s_xr.at[b, u], (g, jnp.maximum(z - 1, 0), tp))

    def x_cross(b, u):
        r = xs(b, tp, u)
        return rc(r, r, s_xxs.at[b, u], s_xxr.at[b, u], (g, z, across))

    def x_cross_in(b, u):
        r = xs(b, across, u)
        return rc(r, r, s_xxs.at[b, u], s_xxr.at[b, u], (g, z, across))

    def x_d2d(b, k, quarter, u):
        r = xs(b, quarter, u)
        return rc(r, r, s_xds.at[b, k, u], s_xdr.at[b, k, u], (g, z, partner))

    for u in range(NS):

        @pl.when(z < SP - 1)
        def _():
            x_right(z, u).start()

        @pl.when(z > 0)
        def _():
            x_left(z, u).start()

    in_q.wait()
    in_k.wait()
    for h in range(2):
        stg[h, 0, :, 0:128] = jnp.concatenate(
            [wqv[:, 64 * h : 64 * h + 64], wkv[:, 64 * h : 64 * h + 64]], axis=1
        )
    for copy in in_w:
        copy.wait()

    def w_half(b, part):
        return WA.at[pl.ds(pl.multiple_of(b * KS + part * KH, KH), KH), :]

    def w_full(b):
        return WA.at[pl.ds(pl.multiple_of(b * KS, KS), KS), :]

    def w_far(h, r):
        return rc(
            stg.at[h, r, pl.ds(pl.multiple_of(g * KH, KH), KH), :],
            w_half(z, g),
            s_ws.at[h, r],
            s_wr.at[z],
            (g, 2 * c + h, 2 * x + r),
        )

    def w_near(h, r):
        return rc(stg.at[h, r], w_full(z), s_ws.at[h, r], s_wr.at[z], (g, z, partner))

    def w_own(h, r):
        return pltpu.make_async_copy(stg.at[h, r], w_full(z), s_wr.at[z])

    def send_w(h):
        for r in range(2):
            zt = 2 * c + h

            @pl.when(zt != z)
            def _():
                w_far(h, r).start()

            @pl.when((zt == z) & (c != r))
            def _():
                w_near(h, r).start()

            @pl.when((zt == z) & (c == r))
            def _():
                w_own(h, r).start()

    send_w(0)
    send_w(1)

    eye = lax.broadcasted_iota(jnp.int32, (R, R), 0) == lax.broadcasted_iota(jnp.int32, (R, R), 1)

    def to_row(col):
        return jnp.broadcast_to(
            jnp.sum(jnp.where(eye, jnp.broadcast_to(col, (R, R)), 0.0), axis=0, keepdims=True), (8, R)
        )

    def to_col(row):
        return jnp.sum(jnp.where(eye, jnp.broadcast_to(row, (R, R)), 0.0), axis=1, keepdims=True)

    def off_far(h):
        return rc(offs.at[h], offr.at[z], s_os.at[h], s_or.at[z], (g, 2 * c + h, 2 * x))

    def off_own(h):
        return pltpu.make_async_copy(offs.at[h], offr.at[z], s_or.at[z])

    ko = key_offset[...].astype(F32)
    for h in range(2):
        offs[h] = jnp.broadcast_to(ko[h : h + 1, :], (8, R))
        own = (2 * c + h == z) & (c == 0)

        @pl.when(own)
        def _():
            off_own(h).start()

        @pl.when(jnp.logical_not(own))
        def _():
            off_far(h).start()

    p_send = rc(prm, prm, s_ps.at[0], s_pr.at[0], (g, z, partner))

    @pl.when(c == mine)
    def _():
        tt = jnp.where(par == 0, conv_taps[:, 0:128], conv_taps[:, 128:256])
        prm[0:taps_n, :] = tt
        prm[32:33, :] = jnp.concatenate([head_gain[0:1, :], head_gain[1:2, :]], axis=1)
        p_send.start()

    def take_z(d):
        for u in range(NS):

            @pl.when(z - d >= 0)
            def _():
                b = z - d
                x_left(b, u).wait_recv()

                @pl.when(z < SP - 1)
                def _():
                    x_right(b, u).start()

                x_cross(b, u).start()
                x_d2d(b, 0, tp, u).start()

            @pl.when(z + d < SP)
            def _():
                b = z + d
                x_left(b, u).wait_recv()

                @pl.when(z > 0)
                def _():
                    x_left(b, u).start()

                x_cross(b, u).start()
                x_d2d(b, 0, tp, u).start()

    def both(d, body):
        for sgn in (-1, 1):

            @pl.when((z + sgn * d >= 0) & (z + sgn * d < SP))
            def _():
                body(z + sgn * d)

    def take_x(d):
        def body(b):
            for u in range(NS):
                x_cross_in(b, u).wait_recv()
                x_d2d(b, 1, across, u).start()

        both(d, body)

    def take_w(d):
        def body(b):
            w = rc(w_half(b, g), w_half(b, g), s_wys.at[b], s_wr.at[b], (1 - g, z, tp))
            w.wait_recv()
            rc(w_half(b, g), w_half(b, g), s_wys.at[b], s_wyr.at[b], (1 - g, z, tp)).start()

        both(d, body)

    take_z(1)
    take_w(1)
    take_x(1)
    take_z(2)
    take_w(2)
    take_x(2)
    take_z(3)
    take_w(3)
    take_x(3)

    @pl.when(c == mine)
    def _():
        pltpu.make_async_copy(w_full(z), w_full(z), s_wr.at[z]).wait()

    @pl.when(c != mine)
    def _():
        rc(w_full(z), w_full(z), s_ws.at[0, 0], s_wr.at[z], (g, z, partner)).wait_recv()
        p_send.wait_recv()

    for d in range(1, SP):
        for sgn in (-1, 1):

            @pl.when((z + sgn * d >= 0) & (z + sgn * d < SP))
            def _():
                b = z + sgn * d
                for u in range(NS):
                    x_d2d(b, 0, partner, u).wait_recv()
                    x_d2d(b, 1, diag, u).wait_recv()
                rc(
                    w_half(b, 1 - g), w_half(b, 1 - g), s_wys.at[b], s_wyr.at[b], (1 - g, z, tp)
                ).wait_recv()

    for b in range(SP):
        proj[b * R : b * R + R, :] = jnp.dot(
            X[b * R : b * R + R, :], WA[...], preferred_element_type=F32
        ).astype(BF16)

    def d_far(t, core):
        buf = ar if core == 0 else cr
        return rc(snd.at[t], buf.at[par], s_ds.at[t], s_dr.at[core, par], (g, t, 2 * x + mine))

    def d_own(t, core):
        buf = ar if core == 0 else cr
        return pltpu.make_async_copy(snd.at[t], buf.at[par], s_dr.at[core, par])

    def l_far(t):
        return rc(lms.at[t], lmr.at[par], s_ls.at[t], s_lr.at[par], (g, t, 2 * x + mine))

    def l_own(t):
        return pltpu.make_async_copy(lms.at[t], lmr.at[par], s_lr.at[par])

    def s_far(t, q):
        return rc(sts.at[t], sr.at[4 * x + z], s_ss.at[t, q], s_sr.at[4 * x + z], (g, t, q))

    def s_own(t):
        return pltpu.make_async_copy(sts.at[t], sr.at[4 * x + z], s_sr.at[4 * x + z])

    @pl.when(c == 0)
    def _():
        for s in range(SP):
            own = (s == z) & (mine == 0)

            @pl.when(own)
            def _():
                pltpu.make_async_copy(offr.at[s], offr.at[s], s_or.at[s]).wait()

            @pl.when(jnp.logical_not(own))
            def _():
                rc(offr.at[s], offr.at[s], s_os.at[0], s_or.at[s], (g, z, partner)).wait_recv()

        row_i = lax.broadcasted_iota(jnp.int32, (R, R), 0)
        col_i = lax.broadcasted_iota(jnp.int32, (R, R), 1)
        upper = jnp.where(row_i >= col_i, 1.0, 0.0).astype(BF16)
        allowed = col_i <= row_i
        lane_ok = (lax.broadcasted_iota(jnp.int32, (R, 128), 1) // 64) == par
        for b in range(SP - 1, -1, -1):
            q = proj[b * R : b * R + R, 0:64]
            acc = jnp.zeros((R, 128), F32)
            mass = jnp.zeros((R, 1), F32)
            carried = jnp.zeros((R, 1), F32)
            for kb in range(b, -1, -1):
                k = proj[kb * R : kb * R + R, 64:128]
                v = proj[kb * R : kb * R + R, 128:256]
                v = jnp.where(lane_ok, v.astype(F32), 0.0).astype(BF16)
                s = (
                    lax.dot_general(q, k, (((1,), (1,)), ((), ())), preferred_element_type=F32)
                    * HD ** (-0.5)
                    + offr[kb, 0:1, :]
                )
                ln = -(jnp.maximum(s, 0.0) + jnp.log1p(jnp.exp(-jnp.abs(s))))
                if kb == b:
                    ln = jnp.where(allowed, ln, 0.0)
                hi = ln.astype(BF16)
                lo = (ln - hi.astype(F32)).astype(BF16)
                incl = (
                    jnp.dot(hi, upper, preferred_element_type=F32)
                    + jnp.dot(lo, upper, preferred_element_type=F32)
                    + carried
                )
                w = jnp.exp(s + incl)
                if kb == b:
                    w = jnp.where(allowed, w, 0.0)
                carried = incl[:, 0:1]
                mass = mass + jnp.sum(w, axis=1, keepdims=True)
                acc = acc + jnp.dot(w.astype(BF16), v, preferred_element_type=F32)
            ms = jnp.sum(acc * acc, axis=1, keepdims=True) / 64
            snd[b] = (acc * lax.rsqrt(ms + norm_eps) * prm[32:33, :]).astype(BF16)
            lms[b] = jnp.log(to_row(mass))
            own = (b == z) & (mine == 0)

            @pl.when(own)
            def _():
                d_own(b, 0).start()
                l_own(b).start()

            @pl.when(jnp.logical_not(own))
            def _():
                d_far(b, 0).start()
                l_far(b).start()

    @pl.when(c == 1)
    def _():
        gp[0:32, :] = jnp.zeros((32, 128), F32)
        gv = proj[:, 0:128].astype(F32)
        gg = proj[:, 128:256].astype(F32)
        gp[32 : 32 + SP * R, :] = (gv * jax.nn.sigmoid(gg)).astype(BF16).astype(F32)
        for b in range(SP):
            conv = jnp.zeros((R, 128), F32)
            for j in range(taps_n):
                first = b * R + 32 - (taps_n - 1) + j
                conv = conv + prm[j : j + 1, :] * gp[first : first + R, :]
            snd[b] = conv.astype(BF16)
            sts[b, 0] = to_row(jnp.sum(conv, axis=1, keepdims=True))
            sts[b, 1] = to_row(jnp.sum(conv * conv, axis=1, keepdims=True))
            own = (b == z) & (mine == 1)

            @pl.when(own)
            def _():
                d_own(b, 1).start()

            @pl.when(jnp.logical_not(own))
            def _():
                d_far(b, 1).start()

            for q in range(4):
                self_st = (b == z) & (q == tp)

                @pl.when(self_st)
                def _():
                    s_own(b).start()

                @pl.when(jnp.logical_not(self_st))
                def _():
                    s_far(b, q).start()

    for h in range(2):
        zs = 2 * c + h
        for core in range(2):
            buf = ar if core == 0 else cr
            own = (zs == z) & (c == core)

            @pl.when(own)
            def _():
                pltpu.make_async_copy(buf.at[h], buf.at[h], s_dr.at[core, h]).wait()
                if core == 0:
                    pltpu.make_async_copy(lmr.at[h], lmr.at[h], s_lr.at[h]).wait()

            @pl.when(jnp.logical_not(own))
            def _():
                rc(buf.at[h], buf.at[h], s_ds.at[0], s_dr.at[core, h], (g, z, partner)).wait_recv()
                if core == 0:
                    rc(lmr.at[h], lmr.at[h], s_ls.at[0], s_lr.at[h], (g, z, partner)).wait_recv()

    for xx in range(2):
        for s in range(SP):
            i = 4 * xx + s
            own = (s == z) & (xx == x) & (c == 1)

            @pl.when(own)
            def _():
                pltpu.make_async_copy(sr.at[i], sr.at[i], s_sr.at[i]).wait()

            @pl.when(jnp.logical_not(own))
            def _():
                rc(sr.at[i], sr.at[i], s_ss.at[0, 0], s_sr.at[i], (g, z, partner)).wait_recv()

    log_out[0:1, :] = lmr[0, 0:1, :]
    log_out[1:2, :] = lmr[1, 0:1, :]
    tot = sr[0]
    for i in range(1, 2 * SP):
        tot = tot + sr[i]
    mean = to_col(tot[0, 0:1, :]) / CW
    spread = to_col(tot[1, 0:1, :]) / CW - mean * mean
    inv = lax.rsqrt(spread + norm_eps)
    att = ar[0] + ar[1]
    chans = []
    for h in range(2):
        v = (cr[h].astype(F32) - mean) * inv * channel_gain[:, 128 * h : 128 * h + 128] + channel_bias[
            :, 128 * h : 128 * h + 128
        ]
        chans.append((v * jax.nn.sigmoid(v)).astype(BF16))
    feats = jnp.concatenate([att] + chans, axis=1)
    wo_a.wait()
    wo_c.wait()
    H = R // 2
    n_col = 4
    cw = D // n_col
    away = pl.ds(pl.multiple_of((1 - c) * H, H), H)
    here = pl.ds(pl.multiple_of(c * H, H), H)

    def m_send(k):
        cs = slice(k * cw, (k + 1) * cw)
        return rc(mp.at[away, cs], ma.at[:, cs], s_ms.at[k], s_mr.at[k], (g, z, partner))

    def b_send(k):
        cs = slice(k * cw, (k + 1) * cw)
        return rc(bx.at[:, cs], bxr.at[:, cs], s_bs.at[k], s_br.at[k], (g, z, across))

    for k in range(n_col):
        cs = slice(k * cw, (k + 1) * cw)
        mp[:, cs] = jnp.dot(feats[:, 0:128], woa[:, cs], preferred_element_type=F32) + jnp.dot(
            feats[:, 128:384], woc[:, cs], preferred_element_type=F32
        )
        m_send(k).start()
    for k in range(n_col):
        cs = slice(k * cw, (k + 1) * cw)
        m_send(k).wait_recv()
        bx[:, cs] = (mp[here, cs] + ma[:, cs]).astype(BF16)
        b_send(k).start()
    for k in range(n_col):
        b_send(k).wait_recv()
    tot2 = bx[...].astype(F32) + bxr[...].astype(F32)
    ms = jnp.mean(tot2 * tot2, axis=-1, keepdims=True)
    out[here, :] = (tot2 * lax.rsqrt(ms + norm_eps) * out_gain[...]).astype(BF16)
    e_send = rc(out.at[here, :], out.at[here, :], s_es.at[0], s_er.at[0], (g, z, partner))
    e_send.start()

    for u in range(NS):

        @pl.when(z < SP - 1)
        def _():
            x_right(z, u).wait_send()

        @pl.when(z > 0)
        def _():
            x_left(z, u).wait_send()

    for d in range(1, SP):
        for u in range(NS):

            @pl.when((z - d >= 0) & (z < SP - 1))
            def _():
                x_right(z - d, u).wait_send()

            @pl.when((z + d < SP) & (z > 0))
            def _():
                x_left(z + d, u).wait_send()

        def drain(b):
            for u in range(NS):
                x_cross(b, u).wait_send()
                x_d2d(b, 0, tp, u).wait_send()
                x_d2d(b, 1, across, u).wait_send()
            rc(w_half(b, g), w_half(b, g), s_wys.at[b], s_wyr.at[b], (1 - g, z, tp)).wait_send()

        both(d, drain)

    for h in range(2):
        for r in range(2):
            zt = 2 * c + h

            @pl.when(zt != z)
            def _():
                w_far(h, r).wait_send()

            @pl.when((zt == z) & (c != r))
            def _():
                w_near(h, r).wait_send()

        own = (2 * c + h == z) & (c == 0)

        @pl.when(jnp.logical_not(own))
        def _():
            off_far(h).wait_send()

    @pl.when(c == mine)
    def _():
        p_send.wait_send()

    for t in range(SP):
        for core in range(2):

            @pl.when((c == core) & jnp.logical_not((t == z) & (mine == core)))
            def _():
                d_far(t, core).wait_send()
                if core == 0:
                    l_far(t).wait_send()

        for q in range(4):

            @pl.when((c == 1) & jnp.logical_not((t == z) & (q == tp)))
            def _():
                s_far(t, q).wait_send()

    for k in range(n_col):
        m_send(k).wait_send()
        b_send(k).wait_send()
    e_send.wait()


def split_local(
    tokens,
    norm_gain,
    w_query,
    w_key,
    w_value,
    w_gv,
    w_gg,
    key_offset,
    head_gain,
    conv_taps,
    channel_gain,
    channel_bias,
    w_oa,
    w_oc,
    out_gain,
):
    SP = lax.axis_size("sp")
    R, D = tokens.shape
    KS = w_query.shape[0]
    DMA = pltpu.SemaphoreType.DMA
    vm = pl.BlockSpec(memory_space=pltpu.VMEM)
    hb = pl.BlockSpec(memory_space=pl.ANY)
    V = pltpu.VMEM
    return pl.pallas_call(
        functools.partial(split_kernel, SP),
        out_shape=(
            jax.ShapeDtypeStruct((R, D), BF16),
            jax.ShapeDtypeStruct((2, R), F32),
        ),
        in_specs=[hb, vm] + [hb] * 5 + [vm] * 5 + [hb, hb, vm],
        out_specs=(vm, vm),
        scratch_shapes=[
            V((SP * R, D), BF16),
            V((SP * KS, 256), BF16),
            V((2, 2, KS, 256), BF16),
            V((40, 128), F32),
            V((2, 8, R), F32),
            V((SP, 8, R), F32),
            V((SP * R, 256), BF16),
            V((SP * R + 32, 128), F32),
            V((SP, R, 128), BF16),
            V((SP, 8, R), F32),
            V((SP, 2, 8, R), F32),
            V((2, R, 128), BF16),
            V((2, R, 128), BF16),
            V((2, 8, R), F32),
            V((2 * SP, 2, 8, R), F32),
            V(w_oa.shape, BF16),
            V(w_oc.shape, BF16),
            V((R, D), F32),
            V((R // 2, D), F32),
            V((R // 2, D), BF16),
            V((R // 2, D), BF16),
            DMA((2,)),
            DMA((2, 2)),
            DMA((SP,)),
            DMA((SP,)),
            DMA((SP,)),
            DMA((SP, 2)),
            DMA((SP, 2)),
            DMA((SP, 2)),
            DMA((SP, 2)),
            DMA((SP, 2)),
            DMA((SP, 2, 2)),
            DMA((SP, 2, 2)),
            DMA((1,)),
            DMA((1,)),
            DMA((2,)),
            DMA((SP,)),
            DMA((SP,)),
            DMA((2, 2)),
            DMA((SP,)),
            DMA((2,)),
            DMA((SP, 4)),
            DMA((2 * SP,)),
            DMA((4,)),
            DMA((4,)),
            DMA((4,)),
            DMA((4,)),
            DMA((1,)),
            DMA((1,)),
            V((R, D), BF16),
            V(w_query.shape, BF16),
            V(w_key.shape, BF16),
            DMA((9,)),
        ],
        compiler_params=pltpu.CompilerParams(collective_id=0, has_side_effects=True),
    )(
        tokens,
        norm_gain.reshape(1, -1),
        w_query,
        w_key,
        w_value,
        w_gv,
        w_gg,
        key_offset.T,
        head_gain,
        conv_taps,
        channel_gain.reshape(1, -1),
        channel_bias.reshape(1, -1),
        w_oa,
        w_oc,
        out_gain.reshape(1, -1),
    )


def either(*args):
    tokens, w_query, head_gain, conv_taps = args[0], args[2], args[8], args[9]
    fits = (
        lax.axis_size("grp") == 2
        and lax.axis_size("sp") == 4
        and lax.axis_size("tp") == 4
        and tokens.shape[0] == 128
        and w_query.shape[0] * 4 == tokens.shape[1]
        and head_gain.shape == (2, 64)
        and conv_taps.shape[1] == 256
        and conv_taps.shape[0] <= 32
        and args[3].shape[1] == 128
    )
    return split_local(*args) if fits else local(*args)


def solution(mesh):
    in_specs = (
        P(("grp", "sp"), None),
        P(),
        P("sp", "tp"),
        P("sp", "tp"),
        P("sp", "tp"),
        P("sp", "tp"),
        P("sp", "tp"),
        P(("grp", "sp"), "tp"),
        P("tp", None),
        P(None, "tp"),
        P("tp"),
        P("tp"),
        P("tp", None),
        P("tp", None),
        P(),
    )
    out_specs = (P(("grp", "sp"), None), P("tp", ("grp", "sp")))
    return jax.shard_map(either, mesh=mesh, in_specs=in_specs, out_specs=out_specs, check_vma=False)
```

```python
import functools

import jax
import jax.numpy as jnp
from jax import lax
from jax.experimental import pallas as pl
from jax.experimental.pallas import tpu as pltpu
from jax.sharding import PartitionSpec as P

HD = 64
CW = 1024


norm_eps = 1e-06


def from_behind(value, axis, steps):
    count = lax.axis_size(axis)
    initial, last = (max(0, -steps), min(count, count - steps))
    return lax.ppermute(value, axis, [(source, source + steps) for source in range(initial, last)])


def row_norm(values_in, gain_vec):
    squares = jnp.mean(values_in * values_in, axis=-1, keepdims=True)
    return values_in * lax.rsqrt(squares + norm_eps) * gain_vec


def local(
    tokens,
    norm_gain,
    w_query,
    w_key,
    w_value,
    w_glu_value,
    w_glu_gate,
    key_offset,
    head_gain,
    conv_taps,
    channel_gain,
    channel_bias,
    w_out_attn,
    w_out_conv,
    out_gain,
):
    row_count = tokens.shape[0]
    normed = row_norm(tokens.astype(jnp.float32), norm_gain).astype(jnp.bfloat16)
    weights_in = (w_query, w_key, w_value, w_glu_value, w_glu_gate)
    pieces = (
        lax.all_gather(weights_in[0], "sp", axis=0, tiled=True),
        lax.all_gather(weights_in[1], "sp", axis=0, tiled=True),
        lax.all_gather(weights_in[2], "sp", axis=0, tiled=True),
        lax.all_gather(weights_in[3], "sp", axis=0, tiled=True),
        lax.all_gather(weights_in[4], "sp", axis=0, tiled=True),
    )
    projected = tuple(
        (jnp.dot(normed, shard_piece, preferred_element_type=jnp.float32) for shard_piece in pieces)
    )
    query, key_rows, value_rows, glu_value, glu_gate = [
        summed.astype(jnp.bfloat16) for summed in projected
    ]
    kv_local = key_rows.shape[1] // HD
    group_size = query.shape[1] // key_rows.shape[1]
    heads_local = kv_local * group_size
    all_keys, all_values, all_offsets = (
        lax.all_gather(key_rows, "sp", axis=0, tiled=True),
        lax.all_gather(value_rows, "sp", axis=0, tiled=True),
        lax.all_gather(key_offset, "sp", axis=0, tiled=True),
    )
    sequence_length_total = all_keys.shape[0]
    shard_count = lax.axis_size("sp")
    per_block = 1
    while (
        per_block * 2 <= shard_count
        and shard_count % (per_block * 2) == 0
        and (per_block * 2 * row_count <= 1024)
    ):
        per_block = per_block * 2
    span_len = per_block * row_count
    query_heads = query.reshape(row_count, kv_local, group_size, HD)
    key_heads = all_keys.reshape(sequence_length_total, kv_local, HD)
    value_heads = all_values.reshape(sequence_length_total, kv_local, HD)
    my_index = lax.axis_index("sp")
    query_pos = my_index * row_count + jnp.arange(row_count, dtype=jnp.int32)
    last_block = my_index // per_block
    zeros_mix = jnp.zeros((kv_local, group_size, row_count, HD), jnp.float32)
    zeros_row = jnp.zeros((kv_local, group_size, row_count), jnp.float32)

    def sweep(turn_index, carry):
        head_mix, mass_sum, carried = carry
        first_key = (last_block - turn_index) * span_len
        key_block = lax.dynamic_slice_in_dim(key_heads, first_key, span_len, 0)
        value_block = lax.dynamic_slice_in_dim(value_heads, first_key, span_len, 0)
        offset_block = lax.dynamic_slice_in_dim(all_offsets, first_key, span_len, 0).astype(
            jnp.float32
        )
        offset_block = offset_block.T.reshape(kv_local, group_size, 1, span_len)
        scores = (
            jnp.einsum("qhgd,khd->hgqk", query_heads, key_block, preferred_element_type=jnp.float32)
            * HD ** (-0.5)
            + offset_block
        )
        key_pos = first_key + jnp.arange(span_len, dtype=jnp.int32)
        allowed = key_pos[None, :] <= query_pos[:, None]
        log_not = jnp.where(allowed, jax.nn.log_sigmoid(-scores), 0.0)
        later = lax.cumsum(log_not, axis=3, reverse=True) - log_not + carried[..., None]
        weights = jnp.where(allowed, jnp.exp(jax.nn.log_sigmoid(scores) + later), 0.0)
        head_mix = head_mix + jnp.einsum(
            "hgqk,khd->hgqd",
            weights.astype(jnp.bfloat16),
            value_block,
            preferred_element_type=jnp.float32,
        )
        return (head_mix, mass_sum + jnp.sum(weights, axis=3), carried + jnp.sum(log_not, axis=3))

    head_mix, mass_sum, leftover = lax.fori_loop(
        0, last_block + 1, sweep, (zeros_mix, zeros_row, zeros_row)
    )
    log_mass = jnp.log(mass_sum).reshape(heads_local, row_count)
    head_rows = head_mix.transpose(2, 0, 1, 3).reshape(row_count, heads_local, HD)
    attended = (
        row_norm(head_rows, head_gain).astype(jnp.bfloat16).reshape(row_count, heads_local * HD)
    )
    gated = (glu_value.astype(jnp.float32) * jax.nn.sigmoid(glu_gate.astype(jnp.float32))).astype(
        jnp.bfloat16
    )
    reach_len = conv_taps.shape[0] - 1
    before = from_behind(gated[row_count - reach_len :], "sp", 1)
    padded = jnp.concatenate([before, gated], axis=0).astype(jnp.float32)
    conv_out = jnp.zeros(gated.shape, jnp.float32)
    for tap_index in range(conv_taps.shape[0]):
        conv_out = conv_out + conv_taps[tap_index] * padded[tap_index : tap_index + row_count]
    total_sum, total_squares = lax.psum(
        (jnp.sum(conv_out, axis=1), jnp.sum(conv_out * conv_out, axis=1)), "tp"
    )
    chan_mean = (total_sum / CW)[:, None]
    spread = (total_squares / CW)[:, None] - chan_mean * chan_mean
    centered = conv_out - chan_mean
    channel_out = jax.nn.silu(
        centered * lax.rsqrt(spread + norm_eps) * channel_gain + channel_bias
    ).astype(jnp.bfloat16)
    share = lax.psum_scatter(
        jnp.dot(attended, w_out_attn, preferred_element_type=jnp.float32)
        + jnp.dot(channel_out, w_out_conv, preferred_element_type=jnp.float32),
        "tp",
        scatter_dimension=0,
        tiled=True,
    )
    mixed = lax.all_gather(row_norm(share, out_gain).astype(jnp.bfloat16), "tp", axis=0, tiled=True)
    return (mixed, log_mass)


F32 = jnp.float32
BF16 = jnp.bfloat16
MESH = pl.DeviceIdType.MESH


def split_kernel(
    SP,
    tokens,
    norm_gain,
    w_query,
    w_key,
    w_value,
    w_gv,
    w_gg,
    key_offset,
    head_gain,
    conv_taps,
    channel_gain,
    channel_bias,
    w_oa,
    w_oc,
    out_gain,
    out,
    log_out,
    X,
    WA,
    stg,
    prm,
    offs,
    offr,
    proj,
    gp,
    snd,
    lms,
    sts,
    ar,
    cr,
    lmr,
    sr,
    woa,
    woc,
    mp,
    ma,
    bx,
    bxr,
    s_wo,
    s_ws,
    s_wr,
    s_wys,
    s_wyr,
    s_xl,
    s_xrt,
    s_xr,
    s_xxs,
    s_xxr,
    s_xds,
    s_xdr,
    s_ps,
    s_pr,
    s_os,
    s_or,
    s_ds,
    s_dr,
    s_ls,
    s_lr,
    s_ss,
    s_sr,
    s_ms,
    s_mr,
    s_bs,
    s_br,
    s_es,
    s_er,
    tokv,
    wqv,
    wkv,
    s_in,
):
    g = lax.axis_index("grp")
    z = lax.axis_index("sp")
    tp = lax.axis_index("tp")
    x = tp // 2
    c = tp % 2
    partner = 2 * x + (1 - c)
    across = 2 * (1 - x) + c
    diag = 2 * (1 - x) + (1 - c)
    mine = z // 2
    par = z % 2
    NS = 2
    R = tokens.shape[0]
    D = tokens.shape[1]
    KS = w_query.shape[0]
    KH = KS // 2
    Q = R // 4
    taps_n = conv_taps.shape[0]

    def rc(src, dst, ss, rs, dev):
        return pltpu.make_async_remote_copy(
            src_ref=src, dst_ref=dst, send_sem=ss, recv_sem=rs, device_id=dev, device_id_type=MESH
        )

    def cp(src, dst, i):
        return pltpu.make_async_copy(src, dst, s_in.at[i])

    in_tok = cp(tokens, tokv, 0)
    in_q = cp(w_query, wqv, 1)
    in_k = cp(w_key, wkv, 2)
    in_w = []
    for h in range(2):
        lanes = slice(128 * h, 128 * h + 128)
        in_w.append(cp(w_value, stg.at[h, 0, :, 128:256], 3 + 3 * h))
        in_w.append(cp(w_gv.at[:, lanes], stg.at[h, 1, :, 0:128], 4 + 3 * h))
        in_w.append(cp(w_gg.at[:, lanes], stg.at[h, 1, :, 128:256], 5 + 3 * h))
    wo_a = pltpu.make_async_copy(w_oa, woa, s_wo.at[0])
    wo_c = pltpu.make_async_copy(w_oc, woc, s_wo.at[1])
    for copy in [in_tok, in_q, in_k] + in_w + [wo_a, wo_c]:
        copy.start()

    barrier = pltpu.get_barrier_semaphore()
    for dz in range(SP):
        for dt in range(4):
            if dz == 0 and dt == 0:
                continue
            pl.semaphore_signal(
                barrier, inc=1, device_id=(g, (z + dz) % SP, (tp + dt) % 4), device_id_type=MESH
            )
    pl.semaphore_signal(barrier, inc=1, device_id=(1 - g, z, tp), device_id_type=MESH)

    in_tok.wait()
    t32 = tokv[...].astype(F32)
    sq = jnp.mean(t32 * t32, axis=-1, keepdims=True)
    X[pl.ds(pl.multiple_of(z * R, R), R), :] = (
        t32 * lax.rsqrt(sq + norm_eps) * norm_gain[...]
    ).astype(BF16)
    pl.semaphore_wait(barrier, SP * 4)

    QS = Q // NS

    def xs(block, quarter, u):
        return X.at[pl.ds(pl.multiple_of(block * R + quarter * Q + u * QS, QS), QS), :]

    def x_right(b, u):
        r = xs(b, tp, u)
        return rc(r, r, s_xrt.at[b, u], s_xr.at[b, u], (g, jnp.minimum(z + 1, SP - 1), tp))

    def x_left(b, u):
        r = xs(b, tp, u)
        return rc(r, r, s_xl.at[b, u], s_xr.at[b, u], (g, jnp.maximum(z - 1, 0), tp))

    def x_cross(b, u):
        r = xs(b, tp, u)
        return rc(r, r, s_xxs.at[b, u], s_xxr.at[b, u], (g, z, across))

    def x_cross_in(b, u):
        r = xs(b, across, u)
        return rc(r, r, s_xxs.at[b, u], s_xxr.at[b, u], (g, z, across))

    def x_d2d(b, k, quarter, u):
        r = xs(b, quarter, u)
        return rc(r, r, s_xds.at[b, k, u], s_xdr.at[b, k, u], (g, z, partner))

    for u in range(NS):

        @pl.when(z < SP - 1)
        def _():
            x_right(z, u).start()

        @pl.when(z > 0)
        def _():
            x_left(z, u).start()

    in_q.wait()
    in_k.wait()
    for h in range(2):
        stg[h, 0, :, 0:128] = jnp.concatenate(
            [wqv[:, 64 * h : 64 * h + 64], wkv[:, 64 * h : 64 * h + 64]], axis=1
        )
    for copy in in_w:
        copy.wait()

    KW = KH // NS

    def w_half(b, part, u):
        return WA.at[pl.ds(pl.multiple_of(b * KS + part * KH + u * KW, KW), KW), :]

    def w_full(b):
        return WA.at[pl.ds(pl.multiple_of(b * KS, KS), KS), :]

    def w_far(h, r, u):
        return rc(
            stg.at[h, r, pl.ds(pl.multiple_of(g * KH + u * KW, KW), KW), :],
            w_half(z, g, u),
            s_ws.at[h, r, u],
            s_wr.at[z, u],
            (g, 2 * c + h, 2 * x + r),
        )

    def w_near(h, r):
        return rc(stg.at[h, r], w_full(z), s_ws.at[h, r, 0], s_wr.at[z, 0], (g, z, partner))

    def w_own(h, r):
        return pltpu.make_async_copy(stg.at[h, r], w_full(z), s_wr.at[z, 0])

    def send_w(h):
        for r in range(2):
            zt = 2 * c + h

            @pl.when(zt != z)
            def _():
                for u in range(NS):
                    w_far(h, r, u).start()

            @pl.when((zt == z) & (c != r))
            def _():
                w_near(h, r).start()

            @pl.when((zt == z) & (c == r))
            def _():
                w_own(h, r).start()

    @pl.when(2 * z >= SP)
    def _():
        send_w(0)
        send_w(1)

    @pl.when(2 * z < SP)
    def _():
        send_w(1)
        send_w(0)

    eye = lax.broadcasted_iota(jnp.int32, (R, R), 0) == lax.broadcasted_iota(jnp.int32, (R, R), 1)

    def to_row(col):
        return jnp.broadcast_to(
            jnp.sum(jnp.where(eye, jnp.broadcast_to(col, (R, R)), 0.0), axis=0, keepdims=True), (8, R)
        )

    def to_col(row):
        return jnp.sum(jnp.where(eye, jnp.broadcast_to(row, (R, R)), 0.0), axis=1, keepdims=True)

    def off_far(h):
        return rc(offs.at[h], offr.at[z], s_os.at[h], s_or.at[z], (g, 2 * c + h, 2 * x))

    def off_own(h):
        return pltpu.make_async_copy(offs.at[h], offr.at[z], s_or.at[z])

    ko = key_offset[...].astype(F32)
    for h in range(2):
        offs[h] = jnp.broadcast_to(ko[h : h + 1, :], (8, R))
        own = (2 * c + h == z) & (c == 0)

        @pl.when(own)
        def _():
            off_own(h).start()

        @pl.when(jnp.logical_not(own))
        def _():
            off_far(h).start()

    p_send = rc(prm, prm, s_ps.at[0], s_pr.at[0], (g, z, partner))

    @pl.when(c == mine)
    def _():
        tt = jnp.where(par == 0, conv_taps[:, 0:128], conv_taps[:, 128:256])
        prm[0:taps_n, :] = tt
        prm[32:33, :] = jnp.concatenate([head_gain[0:1, :], head_gain[1:2, :]], axis=1)
        p_send.start()

    def take_z(d):
        for u in range(NS):

            @pl.when(z - d >= 0)
            def _():
                b = z - d
                x_left(b, u).wait_recv()

                @pl.when(z < SP - 1)
                def _():
                    x_right(b, u).start()

                x_cross(b, u).start()
                x_d2d(b, 0, tp, u).start()

            @pl.when(z + d < SP)
            def _():
                b = z + d
                x_left(b, u).wait_recv()

                @pl.when(z > 0)
                def _():
                    x_left(b, u).start()

                x_cross(b, u).start()
                x_d2d(b, 0, tp, u).start()

    def both(d, body):
        for sgn in (-1, 1):

            @pl.when((z + sgn * d >= 0) & (z + sgn * d < SP))
            def _():
                body(z + sgn * d)

    def take_x(d):
        def body(b):
            for u in range(NS):
                x_cross_in(b, u).wait_recv()
                x_d2d(b, 1, across, u).start()

        both(d, body)

    def take_w(d):
        def body(b):
            for u in range(NS):
                w = w_half(b, g, u)
                rc(w, w, s_wys.at[b, u], s_wr.at[b, u], (1 - g, z, tp)).wait_recv()
                rc(w, w, s_wys.at[b, u], s_wyr.at[b, u], (1 - g, z, tp)).start()

        both(d, body)

    take_z(1)
    take_w(1)
    take_z(2)
    take_x(1)
    take_w(2)
    take_z(3)
    take_x(2)
    take_w(3)
    take_x(3)

    @pl.when(c == mine)
    def _():
        pltpu.make_async_copy(w_full(z), w_full(z), s_wr.at[z, 0]).wait()

    @pl.when(c != mine)
    def _():
        rc(w_full(z), w_full(z), s_ws.at[0, 0, 0], s_wr.at[z, 0], (g, z, partner)).wait_recv()
        p_send.wait_recv()

    for d in range(1, SP):
        for sgn in (-1, 1):

            @pl.when((z + sgn * d >= 0) & (z + sgn * d < SP))
            def _():
                b = z + sgn * d
                for u in range(NS):
                    x_d2d(b, 0, partner, u).wait_recv()
                    x_d2d(b, 1, diag, u).wait_recv()
                for u in range(NS):
                    w = w_half(b, 1 - g, u)
                    rc(w, w, s_wys.at[b, u], s_wyr.at[b, u], (1 - g, z, tp)).wait_recv()

    for b in range(SP):
        proj[b * R : b * R + R, :] = jnp.dot(
            X[b * R : b * R + R, :], WA[...], preferred_element_type=F32
        ).astype(BF16)

    def d_far(t, core):
        buf = ar if core == 0 else cr
        return rc(snd.at[t], buf.at[par], s_ds.at[t], s_dr.at[core, par], (g, t, 2 * x + mine))

    def d_own(t, core):
        buf = ar if core == 0 else cr
        return pltpu.make_async_copy(snd.at[t], buf.at[par], s_dr.at[core, par])

    def l_far(t):
        return rc(lms.at[t], lmr.at[par], s_ls.at[t], s_lr.at[par], (g, t, 2 * x + mine))

    def l_own(t):
        return pltpu.make_async_copy(lms.at[t], lmr.at[par], s_lr.at[par])

    def s_far(t, q):
        return rc(sts.at[t], sr.at[4 * x + z], s_ss.at[t, q], s_sr.at[4 * x + z], (g, t, q))

    def s_own(t):
        return pltpu.make_async_copy(sts.at[t], sr.at[4 * x + z], s_sr.at[4 * x + z])

    @pl.when(c == 0)
    def _():
        for s in range(SP):
            own = (s == z) & (mine == 0)

            @pl.when(own)
            def _():
                pltpu.make_async_copy(offr.at[s], offr.at[s], s_or.at[s]).wait()

            @pl.when(jnp.logical_not(own))
            def _():
                rc(offr.at[s], offr.at[s], s_os.at[0], s_or.at[s], (g, z, partner)).wait_recv()

        row_i = lax.broadcasted_iota(jnp.int32, (R, R), 0)
        col_i = lax.broadcasted_iota(jnp.int32, (R, R), 1)
        upper = jnp.where(row_i >= col_i, 1.0, 0.0).astype(BF16)
        allowed = col_i <= row_i
        lane_ok = (lax.broadcasted_iota(jnp.int32, (R, 128), 1) // 64) == par
        for b in range(SP - 1, -1, -1):
            q = proj[b * R : b * R + R, 0:64]
            acc = jnp.zeros((R, 128), F32)
            mass = jnp.zeros((R, 1), F32)
            carried = jnp.zeros((R, 1), F32)
            for kb in range(b, -1, -1):
                k = proj[kb * R : kb * R + R, 64:128]
                v = proj[kb * R : kb * R + R, 128:256]
                v = jnp.where(lane_ok, v.astype(F32), 0.0).astype(BF16)
                s = (
                    lax.dot_general(q, k, (((1,), (1,)), ((), ())), preferred_element_type=F32)
                    * HD ** (-0.5)
                    + offr[kb, 0:1, :]
                )
                ln = -(jnp.maximum(s, 0.0) + jnp.log1p(jnp.exp(-jnp.abs(s))))
                if kb == b:
                    ln = jnp.where(allowed, ln, 0.0)
                hi = ln.astype(BF16)
                lo = (ln - hi.astype(F32)).astype(BF16)
                incl = (
                    jnp.dot(hi, upper, preferred_element_type=F32)
                    + jnp.dot(lo, upper, preferred_element_type=F32)
                    + carried
                )
                w = jnp.exp(s + incl)
                if kb == b:
                    w = jnp.where(allowed, w, 0.0)
                carried = incl[:, 0:1]
                mass = mass + jnp.sum(w, axis=1, keepdims=True)
                acc = acc + jnp.dot(w.astype(BF16), v, preferred_element_type=F32)
            ms = jnp.sum(acc * acc, axis=1, keepdims=True) / 64
            snd[b] = (acc * lax.rsqrt(ms + norm_eps) * prm[32:33, :]).astype(BF16)
            lms[b] = jnp.log(to_row(mass))
            own = (b == z) & (mine == 0)

            @pl.when(own)
            def _():
                d_own(b, 0).start()
                l_own(b).start()

            @pl.when(jnp.logical_not(own))
            def _():
                d_far(b, 0).start()
                l_far(b).start()

    @pl.when(c == 1)
    def _():
        gp[0:32, :] = jnp.zeros((32, 128), F32)
        gv = proj[:, 0:128].astype(F32)
        gg = proj[:, 128:256].astype(F32)
        gp[32 : 32 + SP * R, :] = (gv * jax.nn.sigmoid(gg)).astype(BF16).astype(F32)
        for b in range(SP):
            conv = jnp.zeros((R, 128), F32)
            for j in range(taps_n):
                first = b * R + 32 - (taps_n - 1) + j
                conv = conv + prm[j : j + 1, :] * gp[first : first + R, :]
            snd[b] = conv.astype(BF16)
            sts[b, 0] = to_row(jnp.sum(conv, axis=1, keepdims=True))
            sts[b, 1] = to_row(jnp.sum(conv * conv, axis=1, keepdims=True))
            own = (b == z) & (mine == 1)

            @pl.when(own)
            def _():
                d_own(b, 1).start()

            @pl.when(jnp.logical_not(own))
            def _():
                d_far(b, 1).start()

            for q in range(4):
                self_st = (b == z) & (q == tp)

                @pl.when(self_st)
                def _():
                    s_own(b).start()

                @pl.when(jnp.logical_not(self_st))
                def _():
                    s_far(b, q).start()

    for h in range(2):
        zs = 2 * c + h
        for core in range(2):
            buf = ar if core == 0 else cr
            own = (zs == z) & (c == core)

            @pl.when(own)
            def _():
                pltpu.make_async_copy(buf.at[h], buf.at[h], s_dr.at[core, h]).wait()
                if core == 0:
                    pltpu.make_async_copy(lmr.at[h], lmr.at[h], s_lr.at[h]).wait()

            @pl.when(jnp.logical_not(own))
            def _():
                rc(buf.at[h], buf.at[h], s_ds.at[0], s_dr.at[core, h], (g, z, partner)).wait_recv()
                if core == 0:
                    rc(lmr.at[h], lmr.at[h], s_ls.at[0], s_lr.at[h], (g, z, partner)).wait_recv()

    for xx in range(2):
        for s in range(SP):
            i = 4 * xx + s
            own = (s == z) & (xx == x) & (c == 1)

            @pl.when(own)
            def _():
                pltpu.make_async_copy(sr.at[i], sr.at[i], s_sr.at[i]).wait()

            @pl.when(jnp.logical_not(own))
            def _():
                rc(sr.at[i], sr.at[i], s_ss.at[0, 0], s_sr.at[i], (g, z, partner)).wait_recv()

    log_out[0:1, :] = lmr[0, 0:1, :]
    log_out[1:2, :] = lmr[1, 0:1, :]
    tot = sr[0]
    for i in range(1, 2 * SP):
        tot = tot + sr[i]
    mean = to_col(tot[0, 0:1, :]) / CW
    spread = to_col(tot[1, 0:1, :]) / CW - mean * mean
    inv = lax.rsqrt(spread + norm_eps)
    att = ar[0] + ar[1]
    chans = []
    for h in range(2):
        v = (cr[h].astype(F32) - mean) * inv * channel_gain[:, 128 * h : 128 * h + 128] + channel_bias[
            :, 128 * h : 128 * h + 128
        ]
        chans.append((v * jax.nn.sigmoid(v)).astype(BF16))
    feats = jnp.concatenate([att] + chans, axis=1)
    wo_a.wait()
    wo_c.wait()
    H = R // 2
    n_col = 4
    cw = D // n_col
    away = pl.ds(pl.multiple_of((1 - c) * H, H), H)
    here = pl.ds(pl.multiple_of(c * H, H), H)

    def m_send(k):
        cs = slice(k * cw, (k + 1) * cw)
        return rc(mp.at[away, cs], ma.at[:, cs], s_ms.at[k], s_mr.at[k], (g, z, partner))

    def b_send(k):
        cs = slice(k * cw, (k + 1) * cw)
        return rc(bx.at[:, cs], bxr.at[:, cs], s_bs.at[k], s_br.at[k], (g, z, across))

    for k in range(n_col):
        cs = slice(k * cw, (k + 1) * cw)
        mp[:, cs] = jnp.dot(feats[:, 0:128], woa[:, cs], preferred_element_type=F32) + jnp.dot(
            feats[:, 128:384], woc[:, cs], preferred_element_type=F32
        )
        m_send(k).start()
    for k in range(n_col):
        cs = slice(k * cw, (k + 1) * cw)
        m_send(k).wait_recv()
        bx[:, cs] = (mp[here, cs] + ma[:, cs]).astype(BF16)
        b_send(k).start()
    for k in range(n_col):
        b_send(k).wait_recv()
    tot2 = bx[...].astype(F32) + bxr[...].astype(F32)
    ms = jnp.mean(tot2 * tot2, axis=-1, keepdims=True)
    out[here, :] = (tot2 * lax.rsqrt(ms + norm_eps) * out_gain[...]).astype(BF16)
    e_send = rc(out.at[here, :], out.at[here, :], s_es.at[0], s_er.at[0], (g, z, partner))
    e_send.start()

    for u in range(NS):

        @pl.when(z < SP - 1)
        def _():
            x_right(z, u).wait_send()

        @pl.when(z > 0)
        def _():
            x_left(z, u).wait_send()

    for d in range(1, SP):
        for u in range(NS):

            @pl.when((z - d >= 0) & (z < SP - 1))
            def _():
                x_right(z - d, u).wait_send()

            @pl.when((z + d < SP) & (z > 0))
            def _():
                x_left(z + d, u).wait_send()

        def drain(b):
            for u in range(NS):
                x_cross(b, u).wait_send()
                x_d2d(b, 0, tp, u).wait_send()
                x_d2d(b, 1, across, u).wait_send()
            for u in range(NS):
                w = w_half(b, g, u)
                rc(w, w, s_wys.at[b, u], s_wyr.at[b, u], (1 - g, z, tp)).wait_send()

        both(d, drain)

    for h in range(2):
        for r in range(2):
            zt = 2 * c + h

            @pl.when(zt != z)
            def _():
                for u in range(NS):
                    w_far(h, r, u).wait_send()

            @pl.when((zt == z) & (c != r))
            def _():
                w_near(h, r).wait_send()

        own = (2 * c + h == z) & (c == 0)

        @pl.when(jnp.logical_not(own))
        def _():
            off_far(h).wait_send()

    @pl.when(c == mine)
    def _():
        p_send.wait_send()

    for t in range(SP):
        for core in range(2):

            @pl.when((c == core) & jnp.logical_not((t == z) & (mine == core)))
            def _():
                d_far(t, core).wait_send()
                if core == 0:
                    l_far(t).wait_send()

        for q in range(4):

            @pl.when((c == 1) & jnp.logical_not((t == z) & (q == tp)))
            def _():
                s_far(t, q).wait_send()

    for k in range(n_col):
        m_send(k).wait_send()
        b_send(k).wait_send()
    e_send.wait()


def split_local(
    tokens,
    norm_gain,
    w_query,
    w_key,
    w_value,
    w_gv,
    w_gg,
    key_offset,
    head_gain,
    conv_taps,
    channel_gain,
    channel_bias,
    w_oa,
    w_oc,
    out_gain,
):
    SP = lax.axis_size("sp")
    R, D = tokens.shape
    KS = w_query.shape[0]
    DMA = pltpu.SemaphoreType.DMA
    vm = pl.BlockSpec(memory_space=pltpu.VMEM)
    hb = pl.BlockSpec(memory_space=pl.ANY)
    V = pltpu.VMEM
    return pl.pallas_call(
        functools.partial(split_kernel, SP),
        out_shape=(
            jax.ShapeDtypeStruct((R, D), BF16),
            jax.ShapeDtypeStruct((2, R), F32),
        ),
        in_specs=[hb, vm] + [hb] * 5 + [vm] * 5 + [hb, hb, vm],
        out_specs=(vm, vm),
        scratch_shapes=[
            V((SP * R, D), BF16),
            V((SP * KS, 256), BF16),
            V((2, 2, KS, 256), BF16),
            V((40, 128), F32),
            V((2, 8, R), F32),
            V((SP, 8, R), F32),
            V((SP * R, 256), BF16),
            V((SP * R + 32, 128), F32),
            V((SP, R, 128), BF16),
            V((SP, 8, R), F32),
            V((SP, 2, 8, R), F32),
            V((2, R, 128), BF16),
            V((2, R, 128), BF16),
            V((2, 8, R), F32),
            V((2 * SP, 2, 8, R), F32),
            V(w_oa.shape, BF16),
            V(w_oc.shape, BF16),
            V((R, D), F32),
            V((R // 2, D), F32),
            V((R // 2, D), BF16),
            V((R // 2, D), BF16),
            DMA((2,)),
            DMA((2, 2, 2)),
            DMA((SP, 2)),
            DMA((SP, 2)),
            DMA((SP, 2)),
            DMA((SP, 2)),
            DMA((SP, 2)),
            DMA((SP, 2)),
            DMA((SP, 2)),
            DMA((SP, 2)),
            DMA((SP, 2, 2)),
            DMA((SP, 2, 2)),
            DMA((1,)),
            DMA((1,)),
            DMA((2,)),
            DMA((SP,)),
            DMA((SP,)),
            DMA((2, 2)),
            DMA((SP,)),
            DMA((2,)),
            DMA((SP, 4)),
            DMA((2 * SP,)),
            DMA((4,)),
            DMA((4,)),
            DMA((4,)),
            DMA((4,)),
            DMA((1,)),
            DMA((1,)),
            V((R, D), BF16),
            V(w_query.shape, BF16),
            V(w_key.shape, BF16),
            DMA((9,)),
        ],
        compiler_params=pltpu.CompilerParams(collective_id=0, has_side_effects=True),
    )(
        tokens,
        norm_gain.reshape(1, -1),
        w_query,
        w_key,
        w_value,
        w_gv,
        w_gg,
        key_offset.T,
        head_gain,
        conv_taps,
        channel_gain.reshape(1, -1),
        channel_bias.reshape(1, -1),
        w_oa,
        w_oc,
        out_gain.reshape(1, -1),
    )


def either(*args):
    tokens, w_query, head_gain, conv_taps = args[0], args[2], args[8], args[9]
    fits = (
        lax.axis_size("grp") == 2
        and lax.axis_size("sp") == 4
        and lax.axis_size("tp") == 4
        and tokens.shape[0] == 128
        and w_query.shape[0] * 4 == tokens.shape[1]
        and head_gain.shape == (2, 64)
        and conv_taps.shape[1] == 256
        and conv_taps.shape[0] <= 32
        and args[3].shape[1] == 128
    )
    return split_local(*args) if fits else local(*args)


def solution(mesh):
    in_specs = (
        P(("grp", "sp"), None),
        P(),
        P("sp", "tp"),
        P("sp", "tp"),
        P("sp", "tp"),
        P("sp", "tp"),
        P("sp", "tp"),
        P(("grp", "sp"), "tp"),
        P("tp", None),
        P(None, "tp"),
        P("tp"),
        P("tp"),
        P("tp", None),
        P("tp", None),
        P(),
    )
    out_specs = (P(("grp", "sp"), None), P("tp", ("grp", "sp")))
    return jax.shard_map(either, mesh=mesh, in_specs=in_specs, out_specs=out_specs, check_vma=False)
```
